256 devices in a mesh: grp: 2 (over y), sp: 32 (over z, core), tp: 4 (over x).
Axes of the slice: x: 4, y: 2, z: 16, core: 2. Of those that a mesh axis runs over, the one named last changes fastest.
The devices are a block of a 4x16x16 slice.
Arguments:
- query_wide: bfloat16 [32768, 1024], P(('grp', 'sp'), 'tp'), parts along dimension 0, may hold values from -6 to 6
- key_wide: bfloat16 [32768, 1024], P(('grp', 'sp'), 'tp'), parts along dimension 0, may hold values from -6 to 6
- value_wide: bfloat16 [32768, 1024], P(('grp', 'sp'), 'tp'), parts along dimension 0, may hold values from -6 to 6
- decay_wide: float32 [32768, 8], P(('grp', 'sp'), 'tp'), parts along dimension 0, may hold values from -2 to 0, as said below
- query_narrow: bfloat16 [32768, 1024], P(('grp', 'sp'), 'tp'), parts along dimension 0, may hold values from -6 to 6
- key_narrow: bfloat16 [32768, 1024], P(('grp', 'sp'), 'tp'), parts along dimension 0, may hold values from -6 to 6
- value_narrow: bfloat16 [32768, 1024], P(('grp', 'sp'), 'tp'), parts along dimension 0, may hold values from -6 to 6
- decay_narrow: float32 [32768, 16], P(('grp', 'sp'), 'tp'), parts along dimension 0, may hold values from -2 to 0, as said below
- residual: bfloat16 [32768, 2048], P(('grp', 'sp', 'tp')), parts along dimension 0, may hold values from -6 to 6
- out_wide: bfloat16 [1024, 2048], P('tp'), may hold values from -0.125 to 0.125
- out_narrow: bfloat16 [1024, 2048], P('tp'), may hold values from -0.125 to 0.125
- norm_gain: float32 [2048], replicated, may hold values from 0.1 to 1.9
- routes: int32 [32768, 2], P(('grp', 'sp', 'tp')), parts along dimension 0, may hold values from 0 to 31, all different within a row; in each aligned block of 128 rows (0 to 127, 128 to 255, ...) at most 12 rows name the same one
- route_weights: float32 [32768, 2], P(('grp', 'sp', 'tp')), parts along dimension 0, may hold values from 0.1 to 1
- expert_gate: bfloat16 [32, 2048, 2048], P('sp', None, 'tp'), may hold values from -0.375 to 0.375
- expert_up: bfloat16 [32, 2048, 2048], P('sp', None, 'tp'), may hold values from -0.375 to 0.375
- expert_down: bfloat16 [32, 2048, 2048], P('sp', 'tp'), may hold values from -0.03125 to 0.03125
Outputs:
- layer_out: bfloat16 [32768, 2048], P(('grp', 'sp', 'tp')), parts along dimension 0
The draws below stay inside these ranges and needn't reach their ends.
There are 2 independent parts, one for each index of `grp`. The reference program is written for one: setup_inputs(seed, part) draws one part's arguments, and reference() takes and returns one part's arrays. A program takes and returns all parts, laid end to end along the dimension named above; an argument that names none is the same for every part. Nothing has to cross between parts.
Inputs may be any that keep to these rules, and one draw needn't show every extreme that they name: `decay_wide`: every entry is negative. `decay_narrow`: every entry is negative. `routes`: each row names 2 different experts; on the rows of one device no expert is named more than 12 times, a bound that some block reaches.
All inputs are finite; a program needn't handle non-finite values.
Results may differ from the reference program's by a relative error of at most 0.018.
Values may be sent and summed in bfloat16 or wider, within the bound.
A program may use at most 128 MiB of HBM per device.

```python
import math
import jax
import jax.numpy as jnp
import numpy as np
from jax import lax

D = 2048
HEADS_WIDE = 8
HEAD_WIDE = 128
HEADS_NARROW = 16
HEAD_NARROW = 64
FF = 2048
TOP_K = 2
TOK_DEV = 512
STEP_COUNT_FULL = 16384
EXPERTS = 32
ROWS_DEV = 128
CAPACITY = 12
N_SP = 32
N_TP = 4


def decay_draw(key, attention_group_count):
    lookup_vectors = jax.random.split(key, 7)
    fast_share = 0.5
    fast_heads = jax.random.uniform(lookup_vectors[0], (attention_group_count,), jnp.float32) < fast_share
    fast_rate = jax.random.uniform(lookup_vectors[1], (attention_group_count,), jnp.float32, 1.0 / 50.0, 1.0 / 20.0)
    slow_rate = jax.random.uniform(lookup_vectors[2], (attention_group_count,), jnp.float32, 0.1, 0.4) / STEP_COUNT_FULL
    ground_frequency = jnp.where(fast_heads, fast_rate, slow_rate)
    block_count = STEP_COUNT_FULL // TOK_DEV
    block_factor = jnp.exp(jax.random.uniform(lookup_vectors[3], (block_count, attention_group_count), jnp.float32, -0.7, 0.7))
    place_indices = jnp.repeat(block_factor, TOK_DEV, axis=0)
    noise_amplitude = jax.random.uniform(lookup_vectors[4], (STEP_COUNT_FULL, attention_group_count), jnp.float32, 0.5, 1.5)
    spike_place = jax.random.randint(lookup_vectors[5], (2,), 0, STEP_COUNT_FULL)
    spike_magnitude = jax.random.uniform(lookup_vectors[6], (2, attention_group_count), jnp.float32, 0.22, 0.69)
    spike_entry_indices = (jnp.arange(STEP_COUNT_FULL)[:, None] == spike_place[None, :]).astype(jnp.float32)
    return -(ground_frequency[None, :] * place_indices * noise_amplitude) - jnp.dot(spike_entry_indices, spike_magnitude)


def draw_decay_wide(key, part):
    return decay_draw(jax.random.fold_in(key, 11), HEADS_WIDE)


def draw_decay_narrow(key, part):
    return decay_draw(jax.random.fold_in(key, 23), HEADS_NARROW)


def level_of(rng, extent, shards, least, largest):
    loudness, own = 1.0, jax.random.fold_in(rng, 6)
    for position, parts in shards:
        draws = jnp.exp(jax.random.uniform(jax.random.fold_in(own, position), (parts,), jnp.float32, least / len(shards), largest / len(shards)))
        loudness = loudness * jnp.repeat(draws, extent[position] // parts).reshape([-1 if axis == position else 1 for axis in range(len(extent))])
    return loudness


def deal_out(own_key, own, number, rows, number_of, top, most, lean):
    order = jax.random.permutation(own_key, number_of)
    crowded, usual = load_shares(number_of, rows * top, most, lean, True), load_shares(number_of, rows * top, most, lean, False)
    places = jnp.arange(number_of)

    def named(lengths, offset_by):
        used = int((lengths > 0).sum())
        fixed = max(1, used // 4)
        shifted = fixed + (places - fixed + offset_by * (used - fixed)) % max(1, number_of - fixed)
        return jnp.zeros((number_of,), jnp.int32).at[order[jnp.where(places < fixed, places, shifted)]].set(jnp.asarray(lengths, jnp.int32))

    lengths = jnp.where(number % 4 == 0, named(crowded, number // 4), named(usual, number - number // 4 - 1))
    mixed = jax.random.permutation(jax.random.fold_in(own, 3), number_of)
    donor, taker = mixed[0:number_of // 2 * 2:2], mixed[1:number_of // 2 * 2:2]
    room = jnp.minimum(lengths[donor] - 1, most - lengths[taker]) // 2
    room = jnp.where((donor == order[0]) | (taker == order[0]) | (lengths[taker] == 0), 0, jnp.maximum(room, 0))
    shifted = jax.random.randint(jax.random.fold_in(own, 4), (number_of // 2,), 0, 1 << 20) % (room + 1)
    lengths = lengths.at[donor].add(-shifted).at[taker].add(shifted)
    members = jnp.searchsorted(jnp.cumsum(lengths), jnp.arange(rows * top), side="right").astype(jnp.int32)
    table = members.reshape(top, rows).T
    table = table[jax.random.permutation(jax.random.fold_in(own, 1), rows)]
    offset_by = jax.random.randint(jax.random.fold_in(own, 2), (rows, 1), 0, top)
    return jnp.take_along_axis(table, (jnp.arange(top)[None, :] + offset_by) % top, axis=1)


def load_shares(amount, total, limit, slope, full):
    weights = [(1 << 20) // math.isqrt(grade ** slope) + 1 for grade in range(1, amount + 1)]
    largest = limit if full else min(limit, max(-(-total // amount), total * weights[0] // sum(weights)))
    least = 1 if total - largest >= amount - 1 else 0
    counts, rest = [largest] + [least] * (amount - 1), total - largest - least * (amount - 1)
    while rest > 0:
        free = [i for i in range(1, amount) if counts[i] < largest] or [i for i in range(1, amount) if counts[i] < limit]
        pool, remaining = sum([weights[i] for i in free]), rest
        for i in free:
            extra = min(limit - counts[i], max(1, remaining * weights[i] // pool), rest)
            counts[i] = counts[i] + extra
            rest = rest - extra
    return np.array(counts)


def noise(key, shape, width, reach, cuts=(), kind=jnp.bfloat16):
    result = jax.random.normal(key, shape, jnp.float32) * width
    if len(cuts) > 0:
        result = level_of(key, shape, cuts, -0.22, 0.18) * result
    return jnp.clip(result, min=-reach, max=reach).astype(kind)


def setup_inputs(seed: int = 0, part: int = 0) -> dict:
    arg_keys = jax.random.split(jax.random.key(seed), 18)
    part_splits = jax.random.split(jax.random.fold_in(arg_keys[17], part), 18)
    query_wide = noise(part_splits[0], (STEP_COUNT_FULL, HEADS_WIDE * HEAD_WIDE), 1.0, 6.0, ((0, 32), (1, 4)))
    key_wide = noise(part_splits[1], (STEP_COUNT_FULL, HEADS_WIDE * HEAD_WIDE), 1.0, 6.0, ((0, 32), (1, 4)))
    value_wide = noise(part_splits[2], (STEP_COUNT_FULL, HEADS_WIDE * HEAD_WIDE), 1.0, 6.0, ((0, 32), (1, 4)))
    decay_wide = draw_decay_wide(jax.random.fold_in(jax.random.fold_in(arg_keys[17], part), 71), part)
    query_narrow = noise(part_splits[4], (STEP_COUNT_FULL, HEADS_NARROW * HEAD_NARROW), 1.0, 6.0, ((0, 32), (1, 4)))
    key_narrow = noise(part_splits[5], (STEP_COUNT_FULL, HEADS_NARROW * HEAD_NARROW), 1.0, 6.0, ((0, 32), (1, 4)))
    value_narrow = noise(part_splits[6], (STEP_COUNT_FULL, HEADS_NARROW * HEAD_NARROW), 1.0, 6.0, ((0, 32), (1, 4)))
    decay_narrow = draw_decay_narrow(jax.random.fold_in(jax.random.fold_in(arg_keys[17], part), 71), part)
    residual = noise(part_splits[8], (STEP_COUNT_FULL, D), 1.0, 6.0, ((0, 128),))
    out_wide = noise(arg_keys[9], (HEADS_WIDE * HEAD_WIDE, D), (HEADS_WIDE * HEAD_WIDE + HEADS_NARROW * HEAD_NARROW) ** -0.5, 0.125, ((0, 4),))
    out_narrow = noise(arg_keys[10], (HEADS_NARROW * HEAD_NARROW, D), (HEADS_WIDE * HEAD_WIDE + HEADS_NARROW * HEAD_NARROW) ** -0.5, 0.125, ((0, 4),))
    norm_gain = jnp.clip(1.0 + 0.18 * jax.random.normal(arg_keys[11], (D,), jnp.float32), 0.1, 1.9)
    routes_keys = jax.random.split(jax.random.fold_in(part_splits[12], 1), STEP_COUNT_FULL // ROWS_DEV)
    routes_turns = jax.random.permutation(jax.random.fold_in(part_splits[12], 3), STEP_COUNT_FULL // ROWS_DEV)
    routes = jax.vmap(lambda own, number: deal_out(jax.random.fold_in(part_splits[12], 2), own, number, ROWS_DEV, EXPERTS, TOP_K, CAPACITY, 1))(routes_keys, routes_turns).reshape((STEP_COUNT_FULL, TOP_K))
    route_weights = jnp.clip(jnp.exp(math.log(1.0) - 2.3025851 * jax.random.uniform(part_splits[13], (STEP_COUNT_FULL, TOP_K), jnp.float32) ** level_of(part_splits[13], (STEP_COUNT_FULL, TOP_K), ((0, 128),), -0.2, 0.2)), 0.1, 1.0)
    expert_gate = noise(arg_keys[14], (EXPERTS, D, FF), (D // 9) ** -0.5, 0.375, ((0, 32), (2, 4)))
    expert_up = noise(arg_keys[15], (EXPERTS, D, FF), (D // 9) ** -0.5, 0.375, ((0, 32), (2, 4)))
    expert_down = noise(arg_keys[16], (EXPERTS, FF, D), (FF * 16) ** -0.5, 0.03125, ((0, 32), (1, 4)))
    return {"query_wide": query_wide, "key_wide": key_wide, "value_wide": value_wide, "decay_wide": decay_wide, "query_narrow": query_narrow, "key_narrow": key_narrow, "value_narrow": value_narrow, "decay_narrow": decay_narrow, "residual": residual, "out_wide": out_wide, "out_narrow": out_narrow, "norm_gain": norm_gain, "routes": routes, "route_weights": route_weights, "expert_gate": expert_gate, "expert_up": expert_up, "expert_down": expert_down}


norm_eps = 1e-05
clamp_limit = 7.0
swish_alpha = 1.702
rotary_base = 10000.0
highest = lax.Precision.HIGHEST

def rotate(values, positions):
    half_width = values.shape[-1] // 2
    inverse = rotary_base ** (-jnp.arange(half_width, dtype=jnp.float32) / half_width)
    angles = positions[:, None] * inverse[None, :]
    cosine = jnp.cos(angles)[:, None, :]
    sine_part = jnp.sin(angles)[:, None, :]
    lower_half = values[..., :half_width]
    upper_half = values[..., half_width:]
    return jnp.concatenate([lower_half * cosine - upper_half * sine_part, lower_half * sine_part + upper_half * cosine], axis=-1)

def prepare(query_in, key_in, head_width, positions):
    length = query_in.shape[0]
    attention_group_count = query_in.shape[1] // head_width
    query_heads = query_in.astype(jnp.float32).reshape(length, attention_group_count, head_width)
    key_heads = key_in.astype(jnp.float32).reshape(length, attention_group_count, head_width)
    query_rot = rotate(query_heads, positions).astype(jnp.bfloat16)
    key_rot = (rotate(key_heads, positions) * head_width ** (-0.5)).astype(jnp.bfloat16)
    return (query_rot, key_rot)

def group_norm(output_heads):
    center = lax.optimization_barrier(jnp.mean(output_heads, axis=-1, keepdims=True))
    spread = lax.optimization_barrier(jnp.mean(jnp.square(output_heads - center), axis=-1, keepdims=True))
    return (output_heads - center) * lax.rsqrt(spread + norm_eps)

def block_terms(query_f, key_f, value_f, log_decay):
    block_len = query_f.shape[0]
    cumulative = jnp.cumsum(log_decay, axis=0)
    steps_in = jnp.arange(block_len, dtype=jnp.int32)
    causal = steps_in[:, None] >= steps_in[None, :]
    gaps = cumulative.T[:, :, None] - cumulative.T[:, None, :]
    decay_grid = jnp.exp(jnp.where(causal[None], gaps, -jnp.inf))
    scores = jnp.einsum('thd,shd->hts', query_f, key_f, precision=highest) * decay_grid
    inner_part = jnp.einsum('hts,she->the', scores, value_f, precision=highest)
    total_log = cumulative[-1]
    weighted = key_f * jnp.exp(total_log[None, :] - cumulative)[:, :, None]
    state_local = jnp.einsum('shd,she->hde', weighted, value_f, precision=highest)
    return (inner_part, cumulative, total_log, state_local)

def read_carried(query_f, cumulative, state_in):
    return jnp.exp(cumulative)[:, :, None] * jnp.einsum('thd,hde->the', query_f, state_in, precision=highest)

def retain(query_in, key_in, value_in, log_decay, head_width):
    length = query_in.shape[0]
    attention_group_count = query_in.shape[1] // head_width
    positions = jnp.arange(length, dtype=jnp.float32)
    query_rot, key_rot = prepare(query_in, key_in, head_width, positions)
    block_len = math.gcd(length, 128)
    blocks = length // block_len

    def advance(state_now, inputs):
        query_block, key_block, value_block, decay_block = inputs
        query_f = query_block.astype(jnp.float32)
        key_f = key_block.astype(jnp.float32)
        value_f = value_block.astype(jnp.float32)
        inner_part, cumulative, total_log, state_local = block_terms(query_f, key_f, value_f, decay_block)
        output_block = inner_part + read_carried(query_f, cumulative, state_now)
        state_next = jnp.exp(total_log)[:, None, None] * state_now + state_local
        return (state_next, output_block)
    value_heads = value_in.reshape(length, attention_group_count, head_width)
    inputs = (query_rot.reshape(blocks, block_len, attention_group_count, head_width), key_rot.reshape(blocks, block_len, attention_group_count, head_width), value_heads.reshape(blocks, block_len, attention_group_count, head_width), log_decay.reshape(blocks, block_len, attention_group_count))
    final_state, outputs = lax.scan(advance, jnp.zeros((attention_group_count, head_width, head_width), jnp.float32), inputs)
    normed_heads = group_norm(outputs.reshape(length, attention_group_count, head_width))
    return normed_heads.reshape(length, attention_group_count * head_width).astype(jnp.bfloat16)

def activate(gate_pre, up_pre):
    gate_clip = jnp.minimum(gate_pre, clamp_limit)
    up_clip = jnp.clip(up_pre, -clamp_limit, clamp_limit)
    return gate_clip * jax.nn.sigmoid(swish_alpha * gate_clip) * (up_clip + 1.0)

def round_trip(values):
    return lax.optimization_barrier(values.astype(jnp.bfloat16)).astype(jnp.float32)

def moe_reference(normed, routes, route_weights, expert_gate, expert_up, expert_down):
    length = normed.shape[0]
    slot_count = N_SP * N_TP * CAPACITY
    padded = jnp.concatenate([normed, jnp.zeros((1, D), jnp.bfloat16)], axis=0)

    def per_expert(total_rows, inputs):
        expert_index, gate_w, up_w, down_w = inputs
        chosen = routes == expert_index
        hits = jnp.any(chosen, axis=1).astype(jnp.int32)
        weight = lax.optimization_barrier(jnp.sum(jnp.where(chosen, route_weights, 0.0), axis=1))
        weight_pad = jnp.concatenate([weight, jnp.zeros((1,), jnp.float32)])
        rank_in = jnp.cumsum(hits) - hits
        target = jnp.where(hits > 0, rank_in, slot_count).astype(jnp.int32)
        slot_table = jnp.full((slot_count + 1,), length, jnp.int32).at[target].set(jnp.arange(length, dtype=jnp.int32))[:slot_count]
        slot_rows = padded[slot_table]
        gate_pre = jnp.dot(slot_rows, gate_w, preferred_element_type=jnp.float32)
        up_pre = jnp.dot(slot_rows, up_w, preferred_element_type=jnp.float32)
        hidden = activate(gate_pre, up_pre).astype(jnp.bfloat16)
        pieces = hidden.reshape(slot_count, N_TP, FF // N_TP).astype(jnp.float32)
        down_parts = down_w.reshape(N_TP, FF // N_TP, D).astype(jnp.float32)
        partial_value = jnp.einsum('nqf,qfd->qnd', pieces, down_parts)
        summed = lax.optimization_barrier(jnp.sum(round_trip(partial_value), axis=0))
        expert_output = summed.astype(jnp.bfloat16).astype(jnp.float32)
        contrib = expert_output * weight_pad[slot_table][:, None]
        return (total_rows.at[slot_table].add(contrib), None)
    total_rows, unused = lax.scan(per_expert, jnp.zeros((length + 1, D), jnp.float32), (jnp.arange(EXPERTS, dtype=jnp.int32), expert_gate, expert_up, expert_down))
    return total_rows[:length]

def reference(query_wide, key_wide, value_wide, decay_wide, query_narrow, key_narrow, value_narrow, decay_narrow, residual, out_wide, out_narrow, norm_gain, routes, route_weights, expert_gate, expert_up, expert_down):
    mixed_wide = retain(query_wide, key_wide, value_wide, decay_wide, HEAD_WIDE)
    mixed_narrow = retain(query_narrow, key_narrow, value_narrow, decay_narrow, HEAD_NARROW)
    wide_share = HEADS_WIDE * HEAD_WIDE // N_TP
    narrow_share = HEADS_NARROW * HEAD_NARROW // N_TP
    attention = jnp.zeros((STEP_COUNT_FULL, D), jnp.float32)
    for tp_part in range(N_TP):
        wide_cols = slice(tp_part * wide_share, (tp_part + 1) * wide_share)
        narrow_cols = slice(tp_part * narrow_share, (tp_part + 1) * narrow_share)
        partial_value = jnp.dot(mixed_wide[:, wide_cols], out_wide[wide_cols], preferred_element_type=jnp.float32)
        partial_value = partial_value + jnp.dot(mixed_narrow[:, narrow_cols], out_narrow[narrow_cols], preferred_element_type=jnp.float32)
        attention = attention + round_trip(partial_value)
    hidden_state = residual.astype(jnp.float32) + attention
    scale_row = lax.rsqrt(lax.optimization_barrier(jnp.mean(hidden_state * hidden_state, axis=-1, keepdims=True)) + norm_eps)
    normed = (hidden_state * scale_row * norm_gain).astype(jnp.bfloat16)
    routed = moe_reference(normed, routes, route_weights, expert_gate, expert_up, expert_down)
    return (hidden_state + routed).astype(jnp.bfloat16)
```

```python
import functools

import jax
import jax.numpy as jnp
import numpy as np
from jax import lax
from jax.experimental import pallas as pl
from jax.experimental.pallas import tpu as pltpu
from jax.sharding import Mesh
from jax.sharding import PartitionSpec as P

HEAD_WIDE = 128
HEAD_NARROW = 64
TOP_K = 2
SP = ("sp_0", "sp_1")
GRP_SP = ("grp", "sp_0", "sp_1")
GRP_SP_TP = ("grp", "sp_0", "sp_1", "tp")


norm_eps = 1e-05
clamp_limit = 7.0
swish_alpha = 1.702
rotary_base = 10000.0


def filled_with(value, identity):
    return jax.tree.map(
        lambda a, e: jnp.broadcast_to(jnp.asarray(e, a.dtype), a.shape), value, identity
    )


def prefix_by_axis(value, axes, combine, identity):
    before = start = filled_with(value, identity)
    total = value
    for axis in reversed(axes):
        length, mine = (lax.axis_size(axis), lax.axis_index(axis))
        pieces = jax.tree.map(
            lambda part, kind: lax.all_gather(part.astype(kind), axis),
            total,
            jax.tree.map(lambda a: jnp.bfloat16 if a.dtype == jnp.float32 else a.dtype, value),
        )
        inside, total = (start, start)
        for k in range(length):
            passed = k < mine
            total = combine(
                total, jax.tree.map(lambda part, own: part[k].astype(own.dtype), pieces, value)
            )
            inside = jax.tree.map(lambda new, old: jnp.where(passed, new, old), total, inside)
        before = combine(inside, before)
    return before


def cut_along(value, dim, length):
    lengths = value.shape
    pieces = value.reshape(*lengths[:dim], length, lengths[dim] // length, *lengths[dim + 1 :])
    return jnp.moveaxis(pieces, dim, 0)


def sent_and_summed(value, axis, dim):
    pieces = cut_along(value, dim, lax.axis_size(axis))
    arrived = lax.all_to_all(pieces, axis, split_axis=0, concat_axis=0, tiled=True)
    return arrived.astype(jnp.float32).sum(axis=0)


def laid_out(pieces, dim):
    pieces = jnp.moveaxis(pieces, 0, dim)
    lengths = pieces.shape
    return pieces.reshape(*lengths[:dim], lengths[dim] * lengths[dim + 1], *lengths[dim + 2 :])


def turned_blocks(pieces, axes, order):
    inside = pieces.shape[1:]
    filled = pieces.reshape(*(lax.axis_size(a) for a in axes), *inside)
    for k in order:
        filled = lax.all_to_all(filled, axes[k], k, k, tiled=True)
    return filled.reshape(-1, *inside)


def core_and_chips(value, groups, order, split_dim, concat_dim):
    length = lax.axis_size(groups[0]) * lax.axis_size(groups[1])
    pieces = cut_along(value, split_dim, length)
    return laid_out(turned_blocks(pieces, groups, order), concat_dim)


def rotate(values, positions):
    half_width = values.shape[-1] // 2
    inverse = rotary_base ** (-jnp.arange(half_width, dtype=jnp.float32) / half_width)
    angles = positions[:, None] * inverse[None, :]
    cosine = jnp.cos(angles)[:, None, :]
    sine_part = jnp.sin(angles)[:, None, :]
    lower_half = values[..., :half_width]
    upper_half = values[..., half_width:]
    return jnp.concatenate(
        [
            lower_half * cosine - upper_half * sine_part,
            lower_half * sine_part + upper_half * cosine,
        ],
        axis=-1,
    )


def group_norm(output_heads):
    center = jnp.mean(output_heads, axis=-1, keepdims=True)
    spread = jnp.mean(jnp.square(output_heads - center), axis=-1, keepdims=True)
    return (output_heads - center) * lax.rsqrt(spread + norm_eps)


def local_terms(query_in, key_in, value_in, log_decay, head_width, positions):
    length = query_in.shape[0]
    attention_group_count = query_in.shape[1] // head_width
    query_heads = query_in.astype(jnp.float32).reshape(length, attention_group_count, head_width)
    key_heads = key_in.astype(jnp.float32).reshape(length, attention_group_count, head_width)
    query_f = rotate(query_heads, positions).astype(jnp.bfloat16).astype(jnp.float32)
    key_f = (
        (rotate(key_heads, positions) * head_width ** (-0.5))
        .astype(jnp.bfloat16)
        .astype(jnp.float32)
    )
    value_f = value_in.reshape(length, attention_group_count, head_width).astype(jnp.float32)
    cumulative = jnp.cumsum(log_decay, axis=0)
    steps_in = jnp.arange(length, dtype=jnp.int32)
    causal = steps_in[:, None] >= steps_in[None, :]
    gaps = cumulative.T[:, :, None] - cumulative.T[:, None, :]
    decay_grid = jnp.exp(jnp.where(causal[None], gaps, -jnp.inf))
    scores = jnp.einsum("thd,shd->hts", query_f, key_f) * decay_grid
    inner_part = jnp.einsum("hts,she->the", scores, value_f)
    total_log = cumulative[-1]
    weighted = key_f * jnp.exp(total_log[None, :] - cumulative)[:, :, None]
    state_local = jnp.einsum("shd,she->hde", weighted, value_f)
    return (query_f, cumulative, inner_part, total_log, state_local)


def finish(parts, state_in):
    query_f, cumulative, inner_part = (parts[0], parts[1], parts[2])
    carried_part = jnp.exp(cumulative)[:, :, None] * jnp.einsum("thd,hde->the", query_f, state_in)
    normed_heads = group_norm(inner_part + carried_part)
    return normed_heads.reshape(normed_heads.shape[0], -1).astype(jnp.bfloat16)


def combine(earlier, later):
    return (
        earlier[0] + later[0],
        jnp.exp(later[0])[:, None, None] * earlier[1] + later[1],
        earlier[2] + later[2],
        jnp.exp(later[2])[:, None, None] * earlier[3] + later[3],
    )


def activate(gate_pre, up_pre):
    gate_clip = jnp.minimum(gate_pre, clamp_limit)
    up_clip = jnp.clip(up_pre, -clamp_limit, clamp_limit)
    return gate_clip * jax.nn.sigmoid(swish_alpha * gate_clip) * (up_clip + 1.0)


QUARTERS = 4
CORES = 2
MESH = pl.DeviceIdType.MESH


def regroup(capacity):
    rows = 4 * QUARTERS * capacity
    table = np.zeros((rows, rows), np.float32)
    for block in range(4):
        for part in range(QUARTERS):
            for row in range(capacity):
                table[
                    (part * 4 + block) * capacity + row, (block * QUARTERS + part) * capacity + row
                ] = 1.0
    return table


def experts_kernel(
    chips,
    send,
    perm,
    perm_back,
    gate_hbm,
    up_hbm,
    down_hbm,
    out,
    gbuf,
    xbuf,
    hbuf,
    pbuf,
    rbuf,
    sbuf,
    ret,
    gate,
    up,
    down,
    load_sem,
    zs,
    zr,
    xs,
    xr,
    ys,
    yr,
    ds,
    dr,
    es,
    er,
    rs,
    rr,
):
    z = lax.axis_index("sp_0")
    c = lax.axis_index("sp_1")
    x = lax.axis_index("tp")
    nx = lax.axis_size("tp")
    me = z * CORES + c
    half = chips // 2
    groups = half
    last = groups - 1
    right = lax.rem(x + 1, nx)
    left = lax.rem(x + nx - 1, nx)
    block_rows = send.shape[1]
    capacity = block_rows // QUARTERS
    rows = 4 * capacity
    width = send.shape[2]
    half_model = QUARTERS * width // 2
    hidden_width = gate.shape[1]

    def remote(src, dst, send_sem, recv_sem, to):
        return pltpu.make_async_remote_copy(
            src_ref=src,
            dst_ref=dst,
            send_sem=send_sem,
            recv_sem=recv_sem,
            device_id=to,
            device_id_type=MESH,
        )

    def at_z(zt, ct):
        return {"sp_0": zt, "sp_1": ct}

    def at_x(xt):
        return {"tp": xt}

    def chip_at(offset):
        return lax.rem(z + offset + chips, chips)

    barrier = pltpu.get_barrier_semaphore()
    pl.semaphore_signal(barrier, inc=1, device_id=at_x(right), device_id_type=MESH)
    pl.semaphore_signal(barrier, inc=1, device_id=at_x(left), device_id_type=MESH)
    pl.semaphore_signal(barrier, inc=1, device_id=at_z(z, 1 - c), device_id_type=MESH)

    @pl.loop(1, chips)
    def _(step):
        for ct in range(CORES):
            pl.semaphore_signal(
                barrier, inc=1, device_id=at_z(chip_at(step), ct), device_id_type=MESH
            )

    loads = [
        pltpu.make_async_copy(gate_hbm, gate, load_sem.at[0]),
        pltpu.make_async_copy(up_hbm, up, load_sem.at[1]),
        pltpu.make_async_copy(down_hbm, down, load_sem.at[2]),
    ]
    for load in loads:
        load.start()
    pl.semaphore_wait(barrier, 3 + CORES * (chips - 1))

    def partner_out():
        return remote(
            send.at[z * CORES + 1 - c], gbuf.at[0, last, c], zs.at[4 * last], zr.at[4 * last],
            at_z(z, 1 - c),
        )

    def far_out(ct):
        zt = chip_at(half)
        return remote(
            send.at[zt * CORES + ct],
            gbuf.at[0, last, 2 + c],
            zs.at[4 * last + 2 + ct],
            zr.at[4 * last + 2 + c],
            at_z(zt, ct),
        )

    def near_out(d, sign, ct):
        zt = chip_at(d) if sign == 0 else chip_at(-d)
        return remote(
            send.at[zt * CORES + ct],
            gbuf.at[0, d - 1, 2 * sign + c],
            zs.at[4 * (d - 1) + 2 * sign + ct],
            zr.at[4 * (d - 1) + 2 * sign + c],
            at_z(zt, ct),
        )

    partner_out().start()

    @pl.loop(1, half)
    def _(d):
        for ct in range(CORES):
            for sign in range(2):
                near_out(d, sign, ct).start()

    for ct in range(CORES):
        far_out(ct).start()
    gbuf[0, last, c] = send[me]
    for load in loads:
        load.wait()

    def z_arrived(g, j):
        return remote(send.at[0], gbuf.at[0, g, j], zs.at[0], zr.at[4 * g + j], at_z(z, 1 - c))

    def spread(side, g):
        return remote(
            gbuf.at[0, g],
            gbuf.at[1 + side, g],
            xs.at[side, g],
            xr.at[side, g],
            at_x(right if side == 0 else left),
        )

    def relay(side, g):
        return remote(
            gbuf.at[1 + side, g, pl.ds(2 * side, 2)],
            gbuf.at[3, g, pl.ds(2 * side, 2)],
            ys.at[side, g],
            yr.at[side, g],
            at_x(right if side == 0 else left),
        )

    def stage_a(g):
        @pl.when(g < last)
        def _():
            for j in range(4):
                z_arrived(g, j).wait_recv()

        @pl.when(g == last)
        def _():
            for j in (0, 2, 3):
                z_arrived(g, j).wait_recv()

        for side in range(2):
            spread(side, g).start()

    def stage_b(g):
        for side in range(2):
            spread(side, g).wait_recv()
            relay(side, g).start()

    def far_half(side, g):
        return remote(
            pbuf.at[g, 3, side],
            rbuf.at[side, g],
            ds.at[side, g],
            dr.at[side, g],
            at_x(right if side == 0 else left),
        )

    def plain_half(side, g):
        return remote(
            pbuf.at[g, 2 - side, 1 - side],
            sbuf.at[side, 1 - side, g],
            es.at[side, 0, g],
            er.at[side, 0, g],
            at_x(right if side == 0 else left),
        )

    def added_half(side, g):
        return remote(
            pbuf.at[g, 2 - side, side],
            sbuf.at[side, side, g],
            es.at[side, 1, g],
            er.at[side, 1, g],
            at_x(right if side == 0 else left),
        )

    def stage_c(g):
        for side in range(2):
            relay(side, g).wait_recv()
        for part in range(4):
            block = gbuf[part, g].reshape(4 * block_rows, width)
            turned = jnp.dot(perm[...], block, preferred_element_type=jnp.float32).astype(
                jnp.bfloat16
            )
            for q in range(QUARTERS):
                xbuf[pl.ds(part * rows, rows), pl.ds(q * width, width)] = turned[
                    q * rows : (q + 1) * rows
                ]
        step = min(256, hidden_width)

        @pl.loop(0, hidden_width // step)
        def _(n):
            cols = pl.ds(pl.multiple_of(n * step, step), step)
            gate_pre = jnp.dot(xbuf[...], gate[:, cols], preferred_element_type=jnp.float32)
            up_pre = jnp.dot(xbuf[...], up[:, cols], preferred_element_type=jnp.float32)
            hbuf[:, cols] = activate(gate_pre, up_pre).astype(jnp.bfloat16)

        out_step = min(512, half_model)

        @pl.loop(0, half_model // out_step)
        def _(n):
            for side in range(2):
                cols = pl.ds(
                    pl.multiple_of(side * half_model + n * out_step, out_step), out_step
                )
                here = pl.ds(pl.multiple_of(n * out_step, out_step), out_step)
                part_sum = jnp.dot(
                    hbuf[...], down[:, cols], preferred_element_type=jnp.float32
                ).astype(jnp.bfloat16)
                for part in range(4):
                    pbuf[g, part, side, :, here] = part_sum[part * rows : (part + 1) * rows]

        for side in range(2):
            far_half(side, g).start()
        for side in range(2):
            plain_half(side, g).start()

    def stage_e(g):
        for side in range(2):
            far_half(side, g).wait_recv()
            pbuf[g, 2 - side, side] = (
                pbuf[g, 2 - side, side].astype(jnp.float32) + rbuf[side, g].astype(jnp.float32)
            ).astype(jnp.bfloat16)
            added_half(side, g).start()

    def stage_f(g):
        for side in range(2):
            plain_half(side, g).wait_recv()
            added_half(side, g).wait_recv()
        quarters = []
        for h in range(2):
            total = (
                pbuf[g, 0, h].astype(jnp.float32)
                + sbuf[0, h, g].astype(jnp.float32)
                + sbuf[1, h, g].astype(jnp.float32)
            ).astype(jnp.bfloat16)
            quarters += [total[:, :width], total[:, width:]]
        stacked = jnp.concatenate(quarters, axis=0)
        ret[g] = (
            jnp.dot(perm_back[...], stacked, preferred_element_type=jnp.float32)
            .astype(jnp.bfloat16)
            .reshape(4, block_rows, width)
        )

    def near_back(g, sign, cs):
        zt = chip_at(-g - 1) if sign == 0 else chip_at(g + 1)
        return remote(
            ret.at[g, 2 * sign + cs],
            out.at[me],
            rs.at[4 * g + 2 * sign + cs],
            rr.at[4 * g + 2 * sign + c],
            at_z(zt, cs),
        )

    def far_back(cs):
        return remote(
            ret.at[last, 2 + cs],
            out.at[me],
            rs.at[4 * last + 2 + cs],
            rr.at[4 * last + 2 + c],
            at_z(chip_at(half), cs),
        )

    def partner_back():
        return remote(
            ret.at[last, 1 - c], out.at[me], rs.at[4 * last], rr.at[4 * last], at_z(z, 1 - c)
        )

    def stage_h(g):
        @pl.when(g < last)
        def _():
            for cs in range(CORES):
                for sign in range(2):
                    near_back(g, sign, cs).start()

        @pl.when(g == last)
        def _():
            for cs in range(CORES):
                far_back(cs).start()
            partner_back().start()
            out[me] = ret[last, c]

    @pl.loop(0, groups + 4)
    def _(i):
        @pl.when(i >= 4)
        def _():
            stage_f(i - 4)

        @pl.when(i >= groups)
        def _():
            stage_h(i - 4)

        @pl.when((i >= 3) & (i < groups + 3))
        def _():
            stage_e(i - 3)

        @pl.when((i >= 2) & (i < groups + 2))
        def _():
            stage_c(i - 2)

        @pl.when((i >= 1) & (i < groups + 1))
        def _():
            stage_b(i - 1)

        @pl.when(i < groups)
        def _():
            stage_a(i)

        @pl.when(i == last)
        def _():
            @pl.loop(0, groups - 4)
            def _(g):
                stage_h(g)

    partner_out().wait_send()
    partner_back().wait_send()
    partner_back().wait_recv()
    for ct in range(CORES):
        far_out(ct).wait_send()
        far_back(ct).wait_send()

    def back_arrived(g, j):
        return remote(ret.at[0, 0], out.at[0], rs.at[0], rr.at[4 * g + j], at_z(z, 1 - c))

    for j in (2, 3):
        back_arrived(last, j).wait_recv()

    @pl.loop(0, last)
    def _(g):
        for sign in range(2):
            for ct in range(CORES):
                near_out(g + 1, sign, ct).wait_send()
                near_back(g, sign, ct).wait_send()
        for j in range(4):
            back_arrived(g, j).wait_recv()

    @pl.loop(0, groups)
    def _(g):
        for side in range(2):
            spread(side, g).wait_send()
            relay(side, g).wait_send()
            far_half(side, g).wait_send()
            plain_half(side, g).wait_send()
            added_half(side, g).wait_send()


def experts_stage(send, gate, up, down):
    experts, block_rows, width = send.shape
    chips = lax.axis_size("sp_0")
    groups = chips // 2
    capacity = block_rows // QUARTERS
    rows = 4 * capacity
    model_width = QUARTERS * width
    hidden_width = gate.shape[1]
    table = regroup(capacity)
    vmem = pl.BlockSpec(memory_space=pltpu.VMEM)
    hbm = pl.BlockSpec(memory_space=pl.ANY)
    bf16 = jnp.bfloat16
    dma = pltpu.SemaphoreType.DMA
    return pl.pallas_call(
        functools.partial(experts_kernel, chips),
        out_shape=jax.ShapeDtypeStruct(send.shape, bf16),
        in_specs=[vmem, vmem, vmem, hbm, hbm, hbm],
        out_specs=vmem,
        scratch_shapes=[
            pltpu.VMEM((4, groups, 4, block_rows, width), bf16),
            pltpu.VMEM((4 * rows, model_width), bf16),
            pltpu.VMEM((4 * rows, hidden_width), bf16),
            pltpu.VMEM((groups, 4, 2, rows, model_width // 2), bf16),
            pltpu.VMEM((2, groups, rows, model_width // 2), bf16),
            pltpu.VMEM((2, 2, groups, rows, model_width // 2), bf16),
            pltpu.VMEM((groups, 4, block_rows, width), bf16),
            pltpu.VMEM(gate.shape, bf16),
            pltpu.VMEM(up.shape, bf16),
            pltpu.VMEM(down.shape, bf16),
            dma((3,)),
            dma((4 * groups,)),
            dma((4 * groups,)),
            dma((2, groups)),
            dma((2, groups)),
            dma((2, groups)),
            dma((2, groups)),
            dma((2, groups)),
            dma((2, groups)),
            dma((2, 2, groups)),
            dma((2, 2, groups)),
            dma((4 * groups,)),
            dma((4 * groups,)),
        ],
        compiler_params=pltpu.CompilerParams(
            collective_id=0, has_side_effects=True, vmem_limit_bytes=48 * 1024 * 1024
        ),
        name="experts_stage",
    )(send, jnp.asarray(table, bf16), jnp.asarray(table.T, bf16), gate, up, down)


def body(
    query_wide,
    key_wide,
    value_wide,
    decay_wide,
    query_narrow,
    key_narrow,
    value_narrow,
    decay_narrow,
    residual,
    out_wide,
    out_narrow,
    norm_gain,
    routes,
    route_weights,
    expert_gate,
    expert_up,
    expert_down,
):
    length = query_wide.shape[0]
    tp_count = lax.axis_size("tp")
    experts = lax.axis_size(SP)
    model_width = residual.shape[1]
    positions = (lax.axis_index(SP) * length + jnp.arange(length, dtype=jnp.int32)).astype(
        jnp.float32
    )
    wide_parts = local_terms(query_wide, key_wide, value_wide, decay_wide, HEAD_WIDE, positions)
    narrow_parts = local_terms(
        query_narrow, key_narrow, value_narrow, decay_narrow, HEAD_NARROW, positions
    )
    local_states = (wide_parts[3], wide_parts[4], narrow_parts[3], narrow_parts[4])
    identity = tuple((jnp.zeros_like(member) for member in local_states))
    carried = prefix_by_axis(local_states, SP, combine, identity)
    mixed_wide = finish(wide_parts, carried[1])
    mixed_narrow = finish(narrow_parts, carried[3])
    rows_dev = length // tp_count
    attention = sent_and_summed(
        (
            jnp.dot(mixed_wide, out_wide, preferred_element_type=jnp.float32)
            + jnp.dot(mixed_narrow, out_narrow, preferred_element_type=jnp.float32)
        ).astype(jnp.bfloat16),
        "tp",
        0,
    )
    hidden_state = residual.astype(jnp.float32) + attention
    scale_row = lax.rsqrt(jnp.mean(hidden_state * hidden_state, axis=-1, keepdims=True) + norm_eps)
    normed = (hidden_state * scale_row * norm_gain).astype(jnp.bfloat16)
    capacity = max(2, 3 * rows_dev * TOP_K // (2 * experts))
    flat_expert = routes.reshape(-1)
    one_hot = (flat_expert[:, None] == jnp.arange(experts, dtype=jnp.int32)[None, :]).astype(
        jnp.int32
    )
    rank_in = jnp.sum((jnp.cumsum(one_hot, axis=0) - one_hot) * one_hot, axis=1)
    place = (flat_expert * (QUARTERS * capacity) + rank_in).reshape(rows_dev, TOP_K)
    width = model_width // QUARTERS
    places = (
        place[None] + (jnp.arange(QUARTERS, dtype=jnp.int32) * capacity)[:, None, None]
    ).reshape(QUARTERS * rows_dev, TOP_K)
    slots = jnp.arange(experts * QUARTERS * capacity, dtype=jnp.int32)
    chosen = (slots[:, None] == places[None, :, 0]) | (slots[:, None] == places[None, :, 1])
    parted = jnp.concatenate(
        [normed[:, q * width : (q + 1) * width] for q in range(QUARTERS)], axis=0
    )
    send = jnp.dot(
        chosen.astype(jnp.bfloat16), parted, preferred_element_type=jnp.float32
    ).astype(jnp.bfloat16)
    back = experts_stage(
        send.reshape(experts, QUARTERS * capacity, width),
        expert_gate[0],
        expert_up[0],
        expert_down[0],
    ).reshape(experts * QUARTERS * capacity, width)
    routed = jnp.zeros((QUARTERS * rows_dev, width), jnp.float32)
    for k in range(TOP_K):
        picks = (places[:, k][:, None] == slots[None, :]).astype(jnp.bfloat16)
        picked = jnp.dot(picks, back, preferred_element_type=jnp.float32)
        routed = routed + picked * jnp.tile(route_weights[:, k], QUARTERS)[:, None]
    routed = jnp.concatenate(
        [routed[q * rows_dev : (q + 1) * rows_dev] for q in range(QUARTERS)], axis=1
    )
    return (hidden_state + routed).astype(jnp.bfloat16)


def solution(mesh):
    torus = Mesh(
        mesh.devices.reshape(mesh.shape["grp"], 16, 2, mesh.shape["tp"]),
        ("grp", "sp_0", "sp_1", "tp"),
    )
    in_specs = (
        P(GRP_SP, "tp"),
        P(GRP_SP, "tp"),
        P(GRP_SP, "tp"),
        P(GRP_SP, "tp"),
        P(GRP_SP, "tp"),
        P(GRP_SP, "tp"),
        P(GRP_SP, "tp"),
        P(GRP_SP, "tp"),
        P(GRP_SP_TP, None),
        P("tp", None),
        P("tp", None),
        P(),
        P(GRP_SP_TP, None),
        P(GRP_SP_TP, None),
        P(SP, None, "tp"),
        P(SP, None, "tp"),
        P(SP, "tp", None),
    )
    out_specs = P(GRP_SP_TP, None)
    return jax.shard_map(body, mesh=torus, in_specs=in_specs, out_specs=out_specs, check_vma=False)
```

```python
import functools

import jax
import jax.numpy as jnp
import numpy as np
from jax import lax
from jax.experimental import pallas as pl
from jax.experimental.pallas import tpu as pltpu
from jax.sharding import Mesh
from jax.sharding import PartitionSpec as P

HEAD_WIDE = 128
HEAD_NARROW = 64
TOP_K = 2
SP = ("sp_0", "sp_1")
GRP_SP = ("grp", "sp_0", "sp_1")
GRP_SP_TP = ("grp", "sp_0", "sp_1", "tp")


norm_eps = 1e-05
clamp_limit = 7.0
swish_alpha = 1.702
rotary_base = 10000.0


def activate(gate_pre, up_pre):
    gate_clip = jnp.minimum(gate_pre, clamp_limit)
    up_clip = jnp.clip(up_pre, -clamp_limit, clamp_limit)
    return gate_clip * jax.nn.sigmoid(swish_alpha * gate_clip) * (up_clip + 1.0)


QUARTERS = 4
CORES = 2
MESH = pl.DeviceIdType.MESH


def regroup(capacity):
    rows = 4 * QUARTERS * capacity
    table = np.zeros((rows, rows), np.float32)
    for block in range(4):
        for part in range(QUARTERS):
            for row in range(capacity):
                table[
                    (part * 4 + block) * capacity + row, (block * QUARTERS + part) * capacity + row
                ] = 1.0
    return table


def experts_kernel(
    chips,
    send,
    perm,
    perm_back,
    gate_hbm,
    up_hbm,
    down_hbm,
    out,
    gbuf,
    xbuf,
    hbuf,
    pbuf,
    rbuf,
    sbuf,
    ret,
    gate,
    up,
    down,
    load_sem,
    zs,
    zr,
    xs,
    xr,
    ys,
    yr,
    ds,
    dr,
    es,
    er,
    rs,
    rr,
):
    z = lax.axis_index("sp_0")
    c = lax.axis_index("sp_1")
    x = lax.axis_index("tp")
    nx = lax.axis_size("tp")
    me = z * CORES + c
    half = chips // 2
    groups = half
    last = groups - 1
    right = lax.rem(x + 1, nx)
    left = lax.rem(x + nx - 1, nx)
    block_rows = send.shape[1]
    capacity = block_rows // QUARTERS
    rows = 4 * capacity
    width = send.shape[2]
    half_model = QUARTERS * width // 2
    hidden_width = gate.shape[1]

    def remote(src, dst, send_sem, recv_sem, to):
        return pltpu.make_async_remote_copy(
            src_ref=src,
            dst_ref=dst,
            send_sem=send_sem,
            recv_sem=recv_sem,
            device_id=to,
            device_id_type=MESH,
        )

    def at_z(zt, ct):
        return {"sp_0": zt, "sp_1": ct}

    def at_x(xt):
        return {"tp": xt}

    def chip_at(offset):
        return lax.rem(z + offset + chips, chips)

    barrier = pltpu.get_barrier_semaphore()
    pl.semaphore_signal(barrier, inc=1, device_id=at_x(right), device_id_type=MESH)
    pl.semaphore_signal(barrier, inc=1, device_id=at_x(left), device_id_type=MESH)
    pl.semaphore_signal(barrier, inc=1, device_id=at_z(z, 1 - c), device_id_type=MESH)

    @pl.loop(1, chips)
    def _(step):
        for ct in range(CORES):
            pl.semaphore_signal(
                barrier, inc=1, device_id=at_z(chip_at(step), ct), device_id_type=MESH
            )

    loads = [
        pltpu.make_async_copy(gate_hbm, gate, load_sem.at[0]),
        pltpu.make_async_copy(up_hbm, up, load_sem.at[1]),
        pltpu.make_async_copy(down_hbm, down, load_sem.at[2]),
    ]
    for load in loads:
        load.start()
    pl.semaphore_wait(barrier, 3 + CORES * (chips - 1))

    def partner_out():
        return remote(
            send.at[z * CORES + 1 - c], gbuf.at[0, last, c], zs.at[4 * last], zr.at[4 * last],
            at_z(z, 1 - c),
        )

    def far_out(ct):
        zt = chip_at(half)
        return remote(
            send.at[zt * CORES + ct],
            gbuf.at[0, last, 2 + c],
            zs.at[4 * last + 2 + ct],
            zr.at[4 * last + 2 + c],
            at_z(zt, ct),
        )

    def near_out(d, sign, ct):
        zt = chip_at(d) if sign == 0 else chip_at(-d)
        return remote(
            send.at[zt * CORES + ct],
            gbuf.at[0, d - 1, 2 * sign + c],
            zs.at[4 * (d - 1) + 2 * sign + ct],
            zr.at[4 * (d - 1) + 2 * sign + c],
            at_z(zt, ct),
        )

    partner_out().start()

    @pl.loop(1, half)
    def _(d):
        for ct in range(CORES):
            for sign in range(2):
                near_out(d, sign, ct).start()

    for ct in range(CORES):
        far_out(ct).start()
    gbuf[0, last, c] = send[me]
    for load in loads:
        load.wait()

    def z_arrived(g, j):
        return remote(send.at[0], gbuf.at[0, g, j], zs.at[0], zr.at[4 * g + j], at_z(z, 1 - c))

    def spread(side, g):
        return remote(
            gbuf.at[0, g],
            gbuf.at[1 + side, g],
            xs.at[side, g],
            xr.at[side, g],
            at_x(right if side == 0 else left),
        )

    def relay(side, g):
        return remote(
            gbuf.at[1 + side, g, pl.ds(2 * side, 2)],
            gbuf.at[3, g, pl.ds(2 * side, 2)],
            ys.at[side, g],
            yr.at[side, g],
            at_x(right if side == 0 else left),
        )

    def stage_a(g):
        @pl.when(g < last)
        def _():
            for j in range(4):
                z_arrived(g, j).wait_recv()

        @pl.when(g == last)
        def _():
            for j in (0, 2, 3):
                z_arrived(g, j).wait_recv()

        for side in range(2):
            spread(side, g).start()

    def stage_b(g):
        for side in range(2):
            spread(side, g).wait_recv()
            relay(side, g).start()

    def far_half(side, g):
        return remote(
            pbuf.at[g, 3, side],
            rbuf.at[side, g],
            ds.at[side, g],
            dr.at[side, g],
            at_x(right if side == 0 else left),
        )

    def plain_half(side, g):
        return remote(
            pbuf.at[g, 2 - side, 1 - side],
            sbuf.at[side, 1 - side, g],
            es.at[side, 0, g],
            er.at[side, 0, g],
            at_x(right if side == 0 else left),
        )

    def added_half(side, g):
        return remote(
            pbuf.at[g, 2 - side, side],
            sbuf.at[side, side, g],
            es.at[side, 1, g],
            er.at[side, 1, g],
            at_x(right if side == 0 else left),
        )

    def stage_c(g):
        for side in range(2):
            relay(side, g).wait_recv()
        for part in range(4):
            block = gbuf[part, g].reshape(4 * block_rows, width)
            turned = jnp.dot(perm[...], block, preferred_element_type=jnp.float32).astype(
                jnp.bfloat16
            )
            for q in range(QUARTERS):
                xbuf[pl.ds(part * rows, rows), pl.ds(q * width, width)] = turned[
                    q * rows : (q + 1) * rows
                ]
        step = min(256, hidden_width)

        @pl.loop(0, hidden_width // step)
        def _(n):
            cols = pl.ds(pl.multiple_of(n * step, step), step)
            gate_pre = jnp.dot(xbuf[...], gate[:, cols], preferred_element_type=jnp.float32)
            up_pre = jnp.dot(xbuf[...], up[:, cols], preferred_element_type=jnp.float32)
            hbuf[:, cols] = activate(gate_pre, up_pre).astype(jnp.bfloat16)

        out_step = min(512, half_model)

        @pl.loop(0, half_model // out_step)
        def _(n):
            for side in range(2):
                cols = pl.ds(
                    pl.multiple_of(side * half_model + n * out_step, out_step), out_step
                )
                here = pl.ds(pl.multiple_of(n * out_step, out_step), out_step)
                part_sum = jnp.dot(
                    hbuf[...], down[:, cols], preferred_element_type=jnp.float32
                ).astype(jnp.bfloat16)
                for part in range(4):
                    pbuf[g, part, side, :, here] = part_sum[part * rows : (part + 1) * rows]

        for side in range(2):
            far_half(side, g).start()
        for side in range(2):
            plain_half(side, g).start()

    def stage_e(g):
        for side in range(2):
            far_half(side, g).wait_recv()
            pbuf[g, 2 - side, side] = (
                pbuf[g, 2 - side, side].astype(jnp.float32) + rbuf[side, g].astype(jnp.float32)
            ).astype(jnp.bfloat16)
            added_half(side, g).start()

    def stage_f(g):
        for side in range(2):
            plain_half(side, g).wait_recv()
            added_half(side, g).wait_recv()
        quarters = []
        for h in range(2):
            total = (
                pbuf[g, 0, h].astype(jnp.float32)
                + sbuf[0, h, g].astype(jnp.float32)
                + sbuf[1, h, g].astype(jnp.float32)
            ).astype(jnp.bfloat16)
            quarters += [total[:, :width], total[:, width:]]
        stacked = jnp.concatenate(quarters, axis=0)
        ret[g] = (
            jnp.dot(perm_back[...], stacked, preferred_element_type=jnp.float32)
            .astype(jnp.bfloat16)
            .reshape(4, block_rows, width)
        )

    def near_back(g, sign, cs):
        zt = chip_at(-g - 1) if sign == 0 else chip_at(g + 1)
        return remote(
            ret.at[g, 2 * sign + cs],
            out.at[me],
            rs.at[4 * g + 2 * sign + cs],
            rr.at[4 * g + 2 * sign + c],
            at_z(zt, cs),
        )

    def far_back(cs):
        return remote(
            ret.at[last, 2 + cs],
            out.at[me],
            rs.at[4 * last + 2 + cs],
            rr.at[4 * last + 2 + c],
            at_z(chip_at(half), cs),
        )

    def partner_back():
        return remote(
            ret.at[last, 1 - c], out.at[me], rs.at[4 * last], rr.at[4 * last], at_z(z, 1 - c)
        )

    def stage_h(g):
        @pl.when(g < last)
        def _():
            for cs in range(CORES):
                for sign in range(2):
                    near_back(g, sign, cs).start()

        @pl.when(g == last)
        def _():
            for cs in range(CORES):
                far_back(cs).start()
            partner_back().start()
            out[me] = ret[last, c]

    @pl.loop(0, groups + 4)
    def _(i):
        @pl.when(i >= 4)
        def _():
            stage_f(i - 4)

        @pl.when(i >= groups)
        def _():
            stage_h(i - 4)

        @pl.when((i >= 3) & (i < groups + 3))
        def _():
            stage_e(i - 3)

        @pl.when((i >= 2) & (i < groups + 2))
        def _():
            stage_c(i - 2)

        @pl.when((i >= 1) & (i < groups + 1))
        def _():
            stage_b(i - 1)

        @pl.when(i < groups)
        def _():
            stage_a(i)

        @pl.when(i == last)
        def _():
            @pl.loop(0, groups - 4)
            def _(g):
                stage_h(g)

    partner_out().wait_send()
    partner_back().wait_send()
    partner_back().wait_recv()
    for ct in range(CORES):
        far_out(ct).wait_send()
        far_back(ct).wait_send()

    def back_arrived(g, j):
        return remote(ret.at[0, 0], out.at[0], rs.at[0], rr.at[4 * g + j], at_z(z, 1 - c))

    for j in (2, 3):
        back_arrived(last, j).wait_recv()

    @pl.loop(0, last)
    def _(g):
        for sign in range(2):
            for ct in range(CORES):
                near_out(g + 1, sign, ct).wait_send()
                near_back(g, sign, ct).wait_send()
        for j in range(4):
            back_arrived(g, j).wait_recv()

    @pl.loop(0, groups)
    def _(g):
        for side in range(2):
            spread(side, g).wait_send()
            relay(side, g).wait_send()
            far_half(side, g).wait_send()
            plain_half(side, g).wait_send()
            added_half(side, g).wait_send()


def experts_stage(send, gate, up, down):
    experts, block_rows, width = send.shape
    chips = lax.axis_size("sp_0")
    groups = chips // 2
    capacity = block_rows // QUARTERS
    rows = 4 * capacity
    model_width = QUARTERS * width
    hidden_width = gate.shape[1]
    table = regroup(capacity)
    vmem = pl.BlockSpec(memory_space=pltpu.VMEM)
    hbm = pl.BlockSpec(memory_space=pl.ANY)
    bf16 = jnp.bfloat16
    dma = pltpu.SemaphoreType.DMA
    return pl.pallas_call(
        functools.partial(experts_kernel, chips),
        out_shape=jax.ShapeDtypeStruct(send.shape, bf16),
        in_specs=[vmem, vmem, vmem, hbm, hbm, hbm],
        out_specs=vmem,
        scratch_shapes=[
            pltpu.VMEM((4, groups, 4, block_rows, width), bf16),
            pltpu.VMEM((4 * rows, model_width), bf16),
            pltpu.VMEM((4 * rows, hidden_width), bf16),
            pltpu.VMEM((groups, 4, 2, rows, model_width // 2), bf16),
            pltpu.VMEM((2, groups, rows, model_width // 2), bf16),
            pltpu.VMEM((2, 2, groups, rows, model_width // 2), bf16),
            pltpu.VMEM((groups, 4, block_rows, width), bf16),
            pltpu.VMEM(gate.shape, bf16),
            pltpu.VMEM(up.shape, bf16),
            pltpu.VMEM(down.shape, bf16),
            dma((3,)),
            dma((4 * groups,)),
            dma((4 * groups,)),
            dma((2, groups)),
            dma((2, groups)),
            dma((2, groups)),
            dma((2, groups)),
            dma((2, groups)),
            dma((2, groups)),
            dma((2, 2, groups)),
            dma((2, 2, groups)),
            dma((4 * groups,)),
            dma((4 * groups,)),
        ],
        compiler_params=pltpu.CompilerParams(
            collective_id=0, has_side_effects=True, vmem_limit_bytes=48 * 1024 * 1024
        ),
        name="experts_stage",
    )(send, jnp.asarray(table, bf16), jnp.asarray(table.T, bf16), gate, up, down)


def in_three(value):
    first = value.astype(jnp.bfloat16)
    rest = value - first.astype(jnp.float32)
    second = rest.astype(jnp.bfloat16)
    third = (rest - second.astype(jnp.float32)).astype(jnp.bfloat16)
    return (first, second, third)


def lanes_of(shape):
    return lax.broadcasted_iota(jnp.int32, shape, len(shape) - 1)


def rows_of(shape):
    return lax.broadcasted_iota(jnp.int32, shape, 0)


def dot_f32(a, b, contract):
    return lax.dot_general(a, b, (contract, ((), ())), preferred_element_type=jnp.float32)


def retention_kernel(
    chips,
    query_wide,
    key_wide,
    value_wide,
    query_narrow,
    key_narrow,
    value_narrow,
    decay,
    decay_t,
    turns,
    out_wide,
    out_narrow,
    residual,
    gain,
    hidden,
    normed,
    qbuf,
    kbuf,
    inner,
    mixed,
    pieces,
    arrived,
    answers,
    states,
    pbuf,
    rbuf,
    sbuf,
    p1s,
    p1r,
    p2s,
    p2r,
    ds,
    dr,
    es,
    er,
):
    z = lax.axis_index("sp_0")
    c = lax.axis_index("sp_1")
    x = lax.axis_index("tp")
    nx = lax.axis_size("tp")
    devices = chips * CORES
    me = z * CORES + c
    right = lax.rem(x + 1, nx)
    left = lax.rem(x + nx - 1, nx)
    length = query_wide.shape[0]
    units = 4
    lane = HEAD_WIDE
    block = min(128, length)
    f32 = jnp.float32
    bf16 = jnp.bfloat16

    def peer(step):
        other = lax.rem(me + step, devices)
        return other, {"sp_0": other // CORES, "sp_1": lax.rem(other, CORES)}

    def at_x(xt):
        return {"tp": xt}

    barrier = pltpu.get_barrier_semaphore()
    pl.semaphore_signal(barrier, inc=1, device_id=at_x(right), device_id_type=MESH)
    pl.semaphore_signal(barrier, inc=1, device_id=at_x(left), device_id_type=MESH)

    @pl.loop(1, devices)
    def _(step):
        pl.semaphore_signal(barrier, inc=1, device_id=peer(step)[1], device_id_type=MESH)

    below = (
        rows_of((length, length)) >= lanes_of((length, length))
    ).astype(f32).astype(bf16)
    cum = sum(dot_f32(below, term, ((1,), (0,))) for term in in_three(decay[...]))
    cum_t = sum(dot_f32(term, below, ((1,), (1,))) for term in in_three(decay_t[...]))

    table_lane = lanes_of((length, lane))
    cos_all = turns[:, :lane]
    sin_all = turns[:, lane:]
    low = table_lane < HEAD_WIDE // 2

    def wide_table(table):
        return jnp.where(low, table, pltpu.roll(table, HEAD_WIDE // 2, 1))

    def narrow_table(table):
        first = pltpu.roll(table, 64, 1)
        twice = jnp.where(table_lane < 32, first, pltpu.roll(first, 32, 1))
        return jnp.where(low, twice, pltpu.roll(twice, 64, 1))

    wide_cos = wide_table(cos_all)
    wide_sin = wide_table(sin_all)
    wide_sin = jnp.where(low, -wide_sin, wide_sin)
    narrow_cos = narrow_table(cos_all)
    narrow_sin = narrow_table(sin_all)
    narrow_low = lax.rem(table_lane, HEAD_NARROW) < HEAD_NARROW // 2
    narrow_sin = jnp.where(narrow_low, -narrow_sin, narrow_sin)

    def turned(source, unit):
        wide = unit < 2
        lanes = slice((unit % 2) * lane, (unit % 2 + 1) * lane)
        values = source[:, lanes].astype(f32)
        if wide:
            return values * wide_cos + pltpu.roll(values, HEAD_WIDE // 2, 1) * wide_sin
        swapped = jnp.where(
            narrow_low,
            pltpu.roll(values, lane - HEAD_NARROW // 2, 1),
            pltpu.roll(values, HEAD_NARROW // 2, 1),
        )
        return values * narrow_cos + swapped * narrow_sin

    def values_of(unit):
        source = value_wide if unit < 2 else value_narrow
        return source[:, (unit % 2) * lane : (unit % 2 + 1) * lane]

    def heads_of(unit):
        return (unit,) if unit < 2 else (2 * unit - 2, 2 * unit - 1)

    def per_lane(unit, column):
        heads = heads_of(unit)
        if len(heads) == 1:
            return column(heads[0])
        shape = (column(heads[0]).shape[0], lane)
        return jnp.where(lanes_of(shape) < HEAD_NARROW, column(heads[0]), column(heads[1]))

    def total_of(head):
        return cum_t[head : head + 1, length - 1 : length]

    unit_shape = (lane, lane)
    unit_low_row = rows_of(unit_shape) < HEAD_NARROW
    unit_low_lane = lanes_of(unit_shape) < HEAD_NARROW
    local = []
    for unit in range(units):
        width = HEAD_WIDE if unit < 2 else HEAD_NARROW
        key = (turned(key_wide if unit < 2 else key_narrow, unit) * width ** (-0.5)).astype(bf16)
        kbuf[unit] = key
        weight = per_lane(unit, lambda h: jnp.exp(total_of(h) - cum[:, h : h + 1]))
        weighted = (key.astype(f32) * weight).astype(bf16)
        state = dot_f32(weighted, values_of(unit), ((0,), (0,)))
        if unit < 2:
            local.append(state)
        else:
            packed = jnp.where(unit_low_row, state, pltpu.roll(state, HEAD_NARROW, 1))
            wide_total = total_of(unit - 2)
            narrow_total = jnp.where(
                unit_low_row, total_of(heads_of(unit)[0]), total_of(heads_of(unit)[1])
            )
            lane_id = lanes_of(unit_shape)
            for position, term in enumerate(
                in_three(jnp.broadcast_to(wide_total, unit_shape)) + in_three(narrow_total)
            ):
                packed = jnp.where(
                    lane_id == HEAD_NARROW + position, term.astype(f32), packed
                )
            local.append(packed)
    piece_rows = 2 * lane // devices
    for unit in range(units):
        here = slice((unit % 2) * (devices // 2), (unit % 2 + 1) * (devices // 2))
        lanes = slice((unit // 2) * lane, (unit // 2 + 1) * lane)
        pieces[here, :, lanes] = local[unit].reshape(devices // 2, piece_rows, lane).astype(bf16)

    pl.semaphore_wait(barrier, 2 + devices - 1)

    def piece_out(step):
        other, where = peer(step)
        return pltpu.make_async_remote_copy(
            src_ref=pieces.at[other],
            dst_ref=arrived.at[me],
            send_sem=p1s.at[step],
            recv_sem=p1r.at[step],
            device_id=where,
            device_id_type=MESH,
        )

    def answer_out(step):
        other, where = peer(step)
        return pltpu.make_async_remote_copy(
            src_ref=answers.at[other],
            dst_ref=states.at[me],
            send_sem=p2s.at[step],
            recv_sem=p2r.at[step],
            device_id=where,
            device_id_type=MESH,
        )

    @pl.loop(1, devices)
    def _(step):
        piece_out(step).start()

    arrived[me] = pieces[me]

    for unit in range(units):
        qbuf[unit] = turned(query_wide if unit < 2 else query_narrow, unit).astype(bf16)

    def within(unit):
        for start in range(0, length, block):
            stop = start + block
            shape = (block, stop)
            causal = rows_of(shape) + start >= lanes_of(shape)
            query = qbuf[unit, start:stop]
            key = kbuf[unit, :stop]
            value = values_of(unit)[:stop]
            outs = []
            for n, head in enumerate(heads_of(unit)):
                own = query
                if unit >= 2:
                    mine = lax.div(lanes_of((block, lane)), HEAD_NARROW) == n
                    own = jnp.where(mine, query.astype(f32), 0.0).astype(bf16)
                scores = dot_f32(own, key, ((1,), (1,)))
                gaps = cum[start:stop, head : head + 1] - cum_t[head : head + 1, :stop]
                faded = scores * jnp.exp(jnp.where(causal, gaps, -jnp.inf))
                outs.append(dot_f32(faded.astype(bf16), value, ((1,), (0,))))
            if unit >= 2:
                outs = [jnp.where(lanes_of((block, lane)) < HEAD_NARROW, outs[0], outs[1])]
            inner[unit, start:stop] = outs[0]

    for unit in range(2):
        within(unit)

    @pl.loop(1, devices)
    def _(step):
        piece_out(step).wait_recv()

    running = jnp.zeros((piece_rows, 2 * lane), f32)
    piece_lane = lanes_of((piece_rows, lane))
    for source in range(devices):
        answers[source] = running.astype(bf16)
        came = arrived[source].astype(f32)
        tail = came[:, lane:]

        def log_at(first):
            terms = (piece_lane >= first) & (piece_lane < first + 3)
            return jnp.sum(jnp.where(terms, tail, 0.0), axis=1, keepdims=True)

        scale = jnp.concatenate(
            [
                jnp.broadcast_to(jnp.exp(log_at(HEAD_NARROW)), piece_lane.shape),
                jnp.broadcast_to(jnp.exp(log_at(HEAD_NARROW + 3)), piece_lane.shape),
            ],
            axis=1,
        )
        running = scale * running + came

    @pl.loop(1, devices)
    def _(step):
        answer_out(step).start()

    states[me] = answers[me]

    for unit in range(2, units):
        within(unit)

    @pl.loop(1, devices)
    def _(step):
        answer_out(step).wait_recv()

    for unit in range(units):
        here = slice((unit % 2) * (devices // 2), (unit % 2 + 1) * (devices // 2))
        lanes = slice((unit // 2) * lane, (unit // 2 + 1) * lane)
        state = states[here, :, lanes].astype(f32).reshape(lane, lane)
        if unit >= 2:
            state = jnp.where(
                unit_low_row,
                jnp.where(unit_low_lane, state, 0.0),
                jnp.where(unit_low_lane, 0.0, pltpu.roll(state, HEAD_NARROW, 1)),
            )
        carried = dot_f32(qbuf[unit], state.astype(bf16), ((1,), (0,)))
        kept = per_lane(unit, lambda h: jnp.exp(cum[:, h : h + 1]))
        value = inner[unit] + kept * carried

        def mean_of(entries):
            if unit < 2:
                return jnp.mean(entries, axis=1, keepdims=True)
            first = jnp.sum(jnp.where(low, entries, 0.0), axis=1, keepdims=True)
            second = jnp.sum(jnp.where(low, 0.0, entries), axis=1, keepdims=True)
            return jnp.where(low, first, second) * (1.0 / HEAD_NARROW)

        centered = value - mean_of(value)
        spread = mean_of(centered * centered)
        mixed[:, unit * lane : (unit + 1) * lane] = (
            centered * lax.rsqrt(spread + norm_eps)
        ).astype(bf16)

    rows_dev = length // nx
    model_width = out_wide.shape[1]
    half_model = model_width // 2

    def x_copy(src, dst, send_sem, recv_sem, side):
        return pltpu.make_async_remote_copy(
            src_ref=src,
            dst_ref=dst,
            send_sem=send_sem,
            recv_sem=recv_sem,
            device_id=at_x(right if side == 0 else left),
            device_id_type=MESH,
        )

    def far_half(side):
        return x_copy(pbuf.at[3, side], rbuf.at[side], ds.at[side], dr.at[side], side)

    def plain_half(side):
        return x_copy(
            pbuf.at[2 - side, 1 - side], sbuf.at[side, 1 - side], es.at[side, 0], er.at[side, 0], side
        )

    def added_half(side):
        return x_copy(
            pbuf.at[2 - side, side], sbuf.at[side, side], es.at[side, 1], er.at[side, 1], side
        )

    out_step = min(512, half_model)

    def project(part, side):
        target = (x, left, right, lax.rem(x + 2, nx))[part]
        own_rows = pl.ds(pl.multiple_of(target * rows_dev, rows_dev), rows_dev)

        @pl.loop(0, half_model // out_step)
        def _(n):
            cols = pl.ds(pl.multiple_of(side * half_model + n * out_step, out_step), out_step)
            here = pl.ds(pl.multiple_of(n * out_step, out_step), out_step)
            both = jnp.dot(
                mixed[own_rows, : 2 * lane], out_wide[:, cols], preferred_element_type=f32
            ) + jnp.dot(
                mixed[own_rows, 2 * lane :], out_narrow[:, cols], preferred_element_type=f32
            )
            pbuf[part, side, :, here] = both.astype(bf16)

    for side in range(2):
        project(3, side)
        far_half(side).start()
    for side in range(2):
        project(2 - side, 1 - side)
        plain_half(side).start()
    for side in range(2):
        project(2 - side, side)
    for side in range(2):
        project(0, side)
    for side in range(2):
        far_half(side).wait_recv()
        pbuf[2 - side, side] = (
            pbuf[2 - side, side].astype(f32) + rbuf[side].astype(f32)
        ).astype(bf16)
        added_half(side).start()
    for side in range(2):
        plain_half(side).wait_recv()
        added_half(side).wait_recv()
    squares = jnp.zeros((rows_dev, 1), f32)
    for h in range(2):
        cols = slice(h * half_model, (h + 1) * half_model)
        stream = residual[:, cols].astype(f32) + (
            pbuf[0, h].astype(f32) + sbuf[0, h].astype(f32) + sbuf[1, h].astype(f32)
        )
        hidden[:, cols] = stream
        squares = squares + jnp.sum(stream * stream, axis=1, keepdims=True)
    scale_row = lax.rsqrt(squares * (1.0 / model_width) + norm_eps)
    normed[...] = (hidden[...] * scale_row * gain[...]).astype(bf16)

    @pl.loop(1, devices)
    def _(step):
        piece_out(step).wait_send()
        answer_out(step).wait_send()

    for side in range(2):
        far_half(side).wait_send()
        plain_half(side).wait_send()
        added_half(side).wait_send()


def retention_stage(
    query_wide,
    key_wide,
    value_wide,
    decay_wide,
    query_narrow,
    key_narrow,
    value_narrow,
    decay_narrow,
    residual,
    out_wide,
    out_narrow,
    norm_gain,
):
    length = query_wide.shape[0]
    chips = lax.axis_size("sp_0")
    devices = chips * CORES
    rows_dev, model_width = residual.shape
    decay = jnp.concatenate(
        [decay_wide, decay_narrow, jnp.zeros((length, 2), jnp.float32)], axis=1
    )
    positions = (lax.axis_index(SP) * length + jnp.arange(length, dtype=jnp.int32)).astype(
        jnp.float32
    )
    inverse = [
        rotary_base ** (-jnp.arange(width // 2, dtype=jnp.float32) / (width // 2))
        for width in (HEAD_WIDE, HEAD_NARROW)
    ]
    inverse = jnp.concatenate(inverse + [jnp.zeros((HEAD_NARROW // 2,), jnp.float32)])
    angles = positions[:, None] * inverse[None, :]
    turns = jnp.concatenate([jnp.cos(angles), jnp.sin(angles)], axis=1)
    vmem = pl.BlockSpec(memory_space=pltpu.VMEM)
    bf16 = jnp.bfloat16
    dma = pltpu.SemaphoreType.DMA
    piece_rows = 2 * HEAD_WIDE // devices
    moved = pltpu.VMEM((devices, piece_rows, 2 * HEAD_WIDE), bf16)
    return pl.pallas_call(
        functools.partial(retention_kernel, chips),
        out_shape=(
            jax.ShapeDtypeStruct(residual.shape, jnp.float32),
            jax.ShapeDtypeStruct(residual.shape, bf16),
        ),
        in_specs=[vmem] * 13,
        out_specs=(vmem, vmem),
        scratch_shapes=[
            pltpu.VMEM((4, length, HEAD_WIDE), bf16),
            pltpu.VMEM((4, length, HEAD_WIDE), bf16),
            pltpu.VMEM((4, length, HEAD_WIDE), jnp.float32),
            pltpu.VMEM((length, 4 * HEAD_WIDE), bf16),
            moved,
            moved,
            moved,
            moved,
            pltpu.VMEM((4, 2, rows_dev, model_width // 2), bf16),
            pltpu.VMEM((2, rows_dev, model_width // 2), bf16),
            pltpu.VMEM((2, 2, rows_dev, model_width // 2), bf16),
            dma((devices,)),
            dma((devices,)),
            dma((devices,)),
            dma((devices,)),
            dma((2,)),
            dma((2,)),
            dma((2, 2)),
            dma((2, 2)),
        ],
        compiler_params=pltpu.CompilerParams(
            collective_id=1, has_side_effects=True, vmem_limit_bytes=40 * 1024 * 1024
        ),
        name="retention_stage",
    )(
        query_wide,
        key_wide,
        value_wide,
        query_narrow,
        key_narrow,
        value_narrow,
        decay,
        decay.T,
        turns,
        out_wide,
        out_narrow,
        residual,
        norm_gain[None, :],
    )


def body(
    query_wide,
    key_wide,
    value_wide,
    decay_wide,
    query_narrow,
    key_narrow,
    value_narrow,
    decay_narrow,
    residual,
    out_wide,
    out_narrow,
    norm_gain,
    routes,
    route_weights,
    expert_gate,
    expert_up,
    expert_down,
):
    experts = lax.axis_size(SP)
    rows_dev, model_width = residual.shape
    hidden_state, normed = retention_stage(
        query_wide,
        key_wide,
        value_wide,
        decay_wide,
        query_narrow,
        key_narrow,
        value_narrow,
        decay_narrow,
        residual,
        out_wide,
        out_narrow,
        norm_gain,
    )
    capacity = max(2, 3 * rows_dev * TOP_K // (2 * experts))
    flat_expert = routes.reshape(-1)
    one_hot = (flat_expert[:, None] == jnp.arange(experts, dtype=jnp.int32)[None, :]).astype(
        jnp.int32
    )
    rank_in = jnp.sum((jnp.cumsum(one_hot, axis=0) - one_hot) * one_hot, axis=1)
    place = (flat_expert * (QUARTERS * capacity) + rank_in).reshape(rows_dev, TOP_K)
    width = model_width // QUARTERS
    places = (
        place[None] + (jnp.arange(QUARTERS, dtype=jnp.int32) * capacity)[:, None, None]
    ).reshape(QUARTERS * rows_dev, TOP_K)
    slots = jnp.arange(experts * QUARTERS * capacity, dtype=jnp.int32)
    chosen = (slots[:, None] == places[None, :, 0]) | (slots[:, None] == places[None, :, 1])
    parted = jnp.concatenate(
        [normed[:, q * width : (q + 1) * width] for q in range(QUARTERS)], axis=0
    )
    send = jnp.dot(
        chosen.astype(jnp.bfloat16), parted, preferred_element_type=jnp.float32
    ).astype(jnp.bfloat16)
    back = experts_stage(
        send.reshape(experts, QUARTERS * capacity, width),
        expert_gate[0],
        expert_up[0],
        expert_down[0],
    ).reshape(experts * QUARTERS * capacity, width)
    routed = jnp.zeros((QUARTERS * rows_dev, width), jnp.float32)
    for k in range(TOP_K):
        picks = (places[:, k][:, None] == slots[None, :]).astype(jnp.bfloat16)
        picked = jnp.dot(picks, back, preferred_element_type=jnp.float32)
        routed = routed + picked * jnp.tile(route_weights[:, k], QUARTERS)[:, None]
    routed = jnp.concatenate(
        [routed[q * rows_dev : (q + 1) * rows_dev] for q in range(QUARTERS)], axis=1
    )
    return (hidden_state + routed).astype(jnp.bfloat16)


def solution(mesh):
    torus = Mesh(
        mesh.devices.reshape(mesh.shape["grp"], 16, 2, mesh.shape["tp"]),
        ("grp", "sp_0", "sp_1", "tp"),
    )
    in_specs = (
        P(GRP_SP, "tp"),
        P(GRP_SP, "tp"),
        P(GRP_SP, "tp"),
        P(GRP_SP, "tp"),
        P(GRP_SP, "tp"),
        P(GRP_SP, "tp"),
        P(GRP_SP, "tp"),
        P(GRP_SP, "tp"),
        P(GRP_SP_TP, None),
        P("tp", None),
        P("tp", None),
        P(),
        P(GRP_SP_TP, None),
        P(GRP_SP_TP, None),
        P(SP, None, "tp"),
        P(SP, None, "tp"),
        P(SP, "tp", None),
    )
    out_specs = P(GRP_SP_TP, None)
    return jax.shard_map(body, mesh=torus, in_specs=in_specs, out_specs=out_specs, check_vma=False)
```

```python
import functools

import jax
import jax.numpy as jnp
import numpy as np
from jax import lax
from jax.experimental import pallas as pl
from jax.experimental.pallas import tpu as pltpu
from jax.sharding import Mesh
from jax.sharding import PartitionSpec as P

HEAD_WIDE = 128
HEAD_NARROW = 64
TOP_K = 2
SP = ("sp_0", "sp_1")
GRP_SP = ("grp", "sp_0", "sp_1")
GRP_SP_TP = ("grp", "sp_0", "sp_1", "tp")


norm_eps = 1e-05
clamp_limit = 7.0
swish_alpha = 1.702
rotary_base = 10000.0


def activate(gate_pre, up_pre):
    gate_clip = jnp.minimum(gate_pre, clamp_limit)
    up_clip = jnp.clip(up_pre, -clamp_limit, clamp_limit)
    return gate_clip * jax.nn.sigmoid(swish_alpha * gate_clip) * (up_clip + 1.0)


QUARTERS = 4
CORES = 2
MESH = pl.DeviceIdType.MESH


def regroup(capacity):
    rows = 4 * QUARTERS * capacity
    table = np.zeros((rows, rows), np.float32)
    for block in range(4):
        for part in range(QUARTERS):
            for row in range(capacity):
                table[
                    (part * 4 + block) * capacity + row, (block * QUARTERS + part) * capacity + row
                ] = 1.0
    return table


def in_three(value):
    first = value.astype(jnp.bfloat16)
    rest = value - first.astype(jnp.float32)
    second = rest.astype(jnp.bfloat16)
    third = (rest - second.astype(jnp.float32)).astype(jnp.bfloat16)
    return (first, second, third)


def lanes_of(shape):
    return lax.broadcasted_iota(jnp.int32, shape, len(shape) - 1)


def rows_of(shape):
    return lax.broadcasted_iota(jnp.int32, shape, 0)


def dot_f32(a, b, contract):
    return lax.dot_general(a, b, (contract, ((), ())), preferred_element_type=jnp.float32)


def layer_kernel(
    chips,
    decay,
    decay_t,
    turns,
    gain,
    routes,
    route_weights,
    perm,
    perm_back,
    query_wide_hbm,
    key_wide_hbm,
    value_wide_hbm,
    query_narrow_hbm,
    key_narrow_hbm,
    value_narrow_hbm,
    out_wide_hbm,
    out_narrow_hbm,
    residual_hbm,
    gate_hbm,
    up_hbm,
    down_hbm,
    out,
    query_wide,
    key_wide,
    value_wide,
    query_narrow,
    key_narrow,
    value_narrow,
    out_wide,
    out_narrow,
    residual,
    gate,
    up,
    down,
    hidden,
    parted,
    chosen,
    picks,
    send,
    back,
    qbuf,
    kbuf,
    inner,
    mixed,
    pieces,
    arrived,
    answers,
    states,
    proj,
    proj_far,
    proj_sum,
    gbuf,
    xbuf,
    hbuf,
    pbuf,
    rbuf,
    sbuf,
    ret,
    load_sem,
    p1s,
    p1r,
    p2s,
    p2r,
    pds,
    pdr,
    pes,
    per,
    zs,
    zr,
    xs,
    xr,
    ys,
    yr,
    ds,
    dr,
    es,
    er,
    rs,
    rr,
):
    z = lax.axis_index("sp_0")
    c = lax.axis_index("sp_1")
    x = lax.axis_index("tp")
    nx = lax.axis_size("tp")
    devices = chips * CORES
    me = z * CORES + c
    right = lax.rem(x + 1, nx)
    left = lax.rem(x + nx - 1, nx)
    length = query_wide.shape[0]
    units = 4
    lane = HEAD_WIDE
    block = min(128, length)
    f32 = jnp.float32
    bf16 = jnp.bfloat16

    def peer(step):
        other = lax.rem(me + step, devices)
        return other, {"sp_0": other // CORES, "sp_1": lax.rem(other, CORES)}

    def at_x(xt):
        return {"tp": xt}

    loads = [
        pltpu.make_async_copy(source, target, load_sem.at[n])
        for n, (source, target) in enumerate(
            (
                (key_wide_hbm, key_wide),
                (key_narrow_hbm, key_narrow),
                (value_wide_hbm, value_wide),
                (value_narrow_hbm, value_narrow),
                (query_wide_hbm, query_wide),
                (query_narrow_hbm, query_narrow),
                (out_wide_hbm, out_wide),
                (out_narrow_hbm, out_narrow),
                (residual_hbm, residual),
                (gate_hbm, gate),
                (up_hbm, up),
                (down_hbm, down),
            )
        )
    ]
    for load in loads[:6]:
        load.start()

    barrier = pltpu.get_barrier_semaphore()
    pl.semaphore_signal(barrier, inc=1, device_id=at_x(right), device_id_type=MESH)
    pl.semaphore_signal(barrier, inc=1, device_id=at_x(left), device_id_type=MESH)

    @pl.loop(1, devices)
    def _(step):
        pl.semaphore_signal(barrier, inc=1, device_id=peer(step)[1], device_id_type=MESH)

    for load in loads[6:]:
        load.start()

    square = (length, length)
    below = (rows_of(square) >= lanes_of(square)).astype(f32).astype(bf16)
    cum = sum(dot_f32(below, term, ((1,), (0,))) for term in in_three(decay[...]))
    cum_t = sum(dot_f32(term, below, ((1,), (1,))) for term in in_three(decay_t[...]))

    table_lane = lanes_of((length, lane))
    cos_all = turns[:, :lane]
    sin_all = turns[:, lane:]
    low = table_lane < HEAD_WIDE // 2

    def wide_table(table):
        return jnp.where(low, table, pltpu.roll(table, HEAD_WIDE // 2, 1))

    def narrow_table(table):
        first = pltpu.roll(table, 64, 1)
        twice = jnp.where(table_lane < 32, first, pltpu.roll(first, 32, 1))
        return jnp.where(low, twice, pltpu.roll(twice, 64, 1))

    wide_cos = wide_table(cos_all)
    wide_sin = wide_table(sin_all)
    wide_sin = jnp.where(low, -wide_sin, wide_sin)
    narrow_cos = narrow_table(cos_all)
    narrow_sin = narrow_table(sin_all)
    narrow_low = lax.rem(table_lane, HEAD_NARROW) < HEAD_NARROW // 2
    narrow_sin = jnp.where(narrow_low, -narrow_sin, narrow_sin)

    def turned(source, unit):
        wide = unit < 2
        lanes = slice((unit % 2) * lane, (unit % 2 + 1) * lane)
        values = source[:, lanes].astype(f32)
        if wide:
            return values * wide_cos + pltpu.roll(values, HEAD_WIDE // 2, 1) * wide_sin
        swapped = jnp.where(
            narrow_low,
            pltpu.roll(values, lane - HEAD_NARROW // 2, 1),
            pltpu.roll(values, HEAD_NARROW // 2, 1),
        )
        return values * narrow_cos + swapped * narrow_sin

    def values_of(unit):
        source = value_wide if unit < 2 else value_narrow
        return source[:, (unit % 2) * lane : (unit % 2 + 1) * lane]

    def heads_of(unit):
        return (unit,) if unit < 2 else (2 * unit - 2, 2 * unit - 1)

    def per_lane(unit, column):
        heads = heads_of(unit)
        if len(heads) == 1:
            return column(heads[0])
        shape = (column(heads[0]).shape[0], lane)
        return jnp.where(lanes_of(shape) < HEAD_NARROW, column(heads[0]), column(heads[1]))

    def total_of(head):
        return cum_t[head : head + 1, length - 1 : length]

    unit_shape = (lane, lane)
    unit_low_row = rows_of(unit_shape) < HEAD_NARROW
    unit_low_lane = lanes_of(unit_shape) < HEAD_NARROW
    for load in loads[:4]:
        load.wait()
    local = []
    for unit in range(units):
        width = HEAD_WIDE if unit < 2 else HEAD_NARROW
        key = (turned(key_wide if unit < 2 else key_narrow, unit) * width ** (-0.5)).astype(bf16)
        kbuf[unit] = key
        weight = per_lane(unit, lambda h: jnp.exp(total_of(h) - cum[:, h : h + 1]))
        weighted = (key.astype(f32) * weight).astype(bf16)
        state = dot_f32(weighted, values_of(unit), ((0,), (0,)))
        if unit < 2:
            local.append(state)
        else:
            packed = jnp.where(unit_low_row, state, pltpu.roll(state, HEAD_NARROW, 1))
            wide_total = total_of(unit - 2)
            narrow_total = jnp.where(
                unit_low_row, total_of(heads_of(unit)[0]), total_of(heads_of(unit)[1])
            )
            lane_id = lanes_of(unit_shape)
            for position, term in enumerate(
                in_three(jnp.broadcast_to(wide_total, unit_shape)) + in_three(narrow_total)
            ):
                packed = jnp.where(
                    lane_id == HEAD_NARROW + position, term.astype(f32), packed
                )
            local.append(packed)
    piece_rows = 2 * lane // devices
    for unit in range(units):
        here = slice((unit % 2) * (devices // 2), (unit % 2 + 1) * (devices // 2))
        lanes = slice((unit // 2) * lane, (unit // 2 + 1) * lane)
        pieces[here, :, lanes] = local[unit].reshape(devices // 2, piece_rows, lane).astype(bf16)

    pl.semaphore_wait(barrier, 2 + devices - 1)

    def piece_out(step):
        other, where = peer(step)
        return pltpu.make_async_remote_copy(
            src_ref=pieces.at[other],
            dst_ref=arrived.at[me],
            send_sem=p1s.at[step],
            recv_sem=p1r.at[step],
            device_id=where,
            device_id_type=MESH,
        )

    def answer_out(step):
        other, where = peer(step)
        return pltpu.make_async_remote_copy(
            src_ref=answers.at[other],
            dst_ref=states.at[me],
            send_sem=p2s.at[step],
            recv_sem=p2r.at[step],
            device_id=where,
            device_id_type=MESH,
        )

    @pl.loop(1, devices)
    def _(step):
        piece_out(step).start()

    arrived[me] = pieces[me]

    for load in loads[4:6]:
        load.wait()
    for unit in range(units):
        qbuf[unit] = turned(query_wide if unit < 2 else query_narrow, unit).astype(bf16)

    def within(unit):
        for start in range(0, length, block):
            stop = start + block
            shape = (block, stop)
            causal = rows_of(shape) + start >= lanes_of(shape)
            query = qbuf[unit, start:stop]
            key = kbuf[unit, :stop]
            value = values_of(unit)[:stop]
            outs = []
            for n, head in enumerate(heads_of(unit)):
                own = query
                if unit >= 2:
                    mine = lax.div(lanes_of((block, lane)), HEAD_NARROW) == n
                    own = jnp.where(mine, query.astype(f32), 0.0).astype(bf16)
                scores = dot_f32(own, key, ((1,), (1,)))
                gaps = cum[start:stop, head : head + 1] - cum_t[head : head + 1, :stop]
                faded = scores * jnp.exp(jnp.where(causal, gaps, -jnp.inf))
                outs.append(dot_f32(faded.astype(bf16), value, ((1,), (0,))))
            if unit >= 2:
                outs = [jnp.where(lanes_of((block, lane)) < HEAD_NARROW, outs[0], outs[1])]
            inner[unit, start:stop] = outs[0]

    for unit in range(2):
        within(unit)

    @pl.loop(1, devices)
    def _(step):
        piece_out(step).wait_recv()

    running = jnp.zeros((piece_rows, 2 * lane), f32)
    piece_lane = lanes_of((piece_rows, lane))
    for source in range(devices):
        answers[source] = running.astype(bf16)
        came = arrived[source].astype(f32)
        tail = came[:, lane:]

        def log_at(first):
            terms = (piece_lane >= first) & (piece_lane < first + 3)
            return jnp.sum(jnp.where(terms, tail, 0.0), axis=1, keepdims=True)

        scale = jnp.concatenate(
            [
                jnp.broadcast_to(jnp.exp(log_at(HEAD_NARROW)), piece_lane.shape),
                jnp.broadcast_to(jnp.exp(log_at(HEAD_NARROW + 3)), piece_lane.shape),
            ],
            axis=1,
        )
        running = scale * running + came

    @pl.loop(1, devices)
    def _(step):
        answer_out(step).start()

    states[me] = answers[me]

    for unit in range(2, units):
        within(unit)

    @pl.loop(1, devices)
    def _(step):
        answer_out(step).wait_recv()

    for unit in range(units):
        here = slice((unit % 2) * (devices // 2), (unit % 2 + 1) * (devices // 2))
        lanes = slice((unit // 2) * lane, (unit // 2 + 1) * lane)
        state = states[here, :, lanes].astype(f32).reshape(lane, lane)
        if unit >= 2:
            state = jnp.where(
                unit_low_row,
                jnp.where(unit_low_lane, state, 0.0),
                jnp.where(unit_low_lane, 0.0, pltpu.roll(state, HEAD_NARROW, 1)),
            )
        carried = dot_f32(qbuf[unit], state.astype(bf16), ((1,), (0,)))
        kept = per_lane(unit, lambda h: jnp.exp(cum[:, h : h + 1]))
        value = inner[unit] + kept * carried

        def mean_of(entries):
            if unit < 2:
                return jnp.mean(entries, axis=1, keepdims=True)
            first = jnp.sum(jnp.where(low, entries, 0.0), axis=1, keepdims=True)
            second = jnp.sum(jnp.where(low, 0.0, entries), axis=1, keepdims=True)
            return jnp.where(low, first, second) * (1.0 / HEAD_NARROW)

        centered = value - mean_of(value)
        spread = mean_of(centered * centered)
        mixed[:, unit * lane : (unit + 1) * lane] = (
            centered * lax.rsqrt(spread + norm_eps)
        ).astype(bf16)

    rows_dev = length // nx
    model_width = out_wide.shape[1]
    proj_half = model_width // 2

    for load in loads[6:9]:
        load.wait()

    def x_copy(src, dst, send_sem, recv_sem, side):
        return pltpu.make_async_remote_copy(
            src_ref=src,
            dst_ref=dst,
            send_sem=send_sem,
            recv_sem=recv_sem,
            device_id=at_x(right if side == 0 else left),
            device_id_type=MESH,
        )

    def proj_far_half(side):
        return x_copy(proj.at[3, side], proj_far.at[side], pds.at[side], pdr.at[side], side)

    def proj_plain_half(side):
        return x_copy(
            proj.at[2 - side, 1 - side], proj_sum.at[side, 1 - side], pes.at[side, 0], per.at[side, 0], side
        )

    def proj_added_half(side):
        return x_copy(
            proj.at[2 - side, side], proj_sum.at[side, side], pes.at[side, 1], per.at[side, 1], side
        )

    out_step = min(512, proj_half)

    def project(part, side):
        target = (x, left, right, lax.rem(x + 2, nx))[part]
        own_rows = pl.ds(pl.multiple_of(target * rows_dev, rows_dev), rows_dev)

        @pl.loop(0, proj_half // out_step)
        def _(n):
            cols = pl.ds(pl.multiple_of(side * proj_half + n * out_step, out_step), out_step)
            here = pl.ds(pl.multiple_of(n * out_step, out_step), out_step)
            both = jnp.dot(
                mixed[own_rows, : 2 * lane], out_wide[:, cols], preferred_element_type=f32
            ) + jnp.dot(
                mixed[own_rows, 2 * lane :], out_narrow[:, cols], preferred_element_type=f32
            )
            proj[part, side, :, here] = both.astype(bf16)

    for side in range(2):
        project(3, side)
        proj_far_half(side).start()
    for side in range(2):
        project(2 - side, 1 - side)
        proj_plain_half(side).start()
    for side in range(2):
        project(2 - side, side)
    for side in range(2):
        project(0, side)
    for side in range(2):
        proj_far_half(side).wait_recv()
        proj[2 - side, side] = (
            proj[2 - side, side].astype(f32) + proj_far[side].astype(f32)
        ).astype(bf16)
        proj_added_half(side).start()
    experts = devices
    one_hots = []
    for k in range(TOP_K):
        wanted = jnp.broadcast_to(routes[:, k : k + 1], (rows_dev, experts))
        one_hots.append((wanted == lanes_of((rows_dev, experts))).astype(f32))
    rows_square = (rows_dev, rows_dev)
    above = (rows_of(rows_square) > lanes_of(rows_square)).astype(f32).astype(bf16)
    diagonal = rows_of(rows_square) == lanes_of(rows_square)
    before = jnp.zeros((1, experts), f32)
    parts = QUARTERS * rows_dev
    slots = send.shape[0] * send.shape[1]
    capacity = send.shape[1] // QUARTERS
    width = send.shape[2]
    picked_rows = []
    for k in range(TOP_K):
        ahead = dot_f32(above, one_hots[k].astype(bf16), ((1,), (0,))) + before
        rank = jnp.sum(ahead * one_hots[k], axis=1, keepdims=True)
        before = before + jnp.sum(one_hots[k], axis=0, keepdims=True)
        place = routes[:, k : k + 1].astype(f32) * float(QUARTERS * capacity) + rank
        across = jnp.sum(
            jnp.where(diagonal, jnp.broadcast_to(place, rows_square), 0.0), axis=0, keepdims=True
        )
        picked_rows.append(
            jnp.concatenate([across + float(q * capacity) for q in range(QUARTERS)], axis=1)
        )
        for q in range(QUARTERS):
            own = slice(q * rows_dev, (q + 1) * rows_dev)
            wanted = jnp.broadcast_to(place + float(q * capacity), (rows_dev, slots))
            picks[k, own] = (
                (wanted == lanes_of((rows_dev, slots)).astype(f32)).astype(f32).astype(bf16)
            )
    step_rows = slots // 4

    @pl.loop(0, 4)
    def _(n):
        first = pl.multiple_of(n * step_rows, step_rows)
        slot = (rows_of((step_rows, parts)) + first).astype(f32)
        hit = (slot == picked_rows[0]) | (slot == picked_rows[1])
        chosen[pl.ds(first, step_rows)] = hit.astype(f32).astype(bf16)

    for side in range(2):
        proj_plain_half(side).wait_recv()
        proj_added_half(side).wait_recv()
    squares = jnp.zeros((rows_dev, 1), f32)
    for h in range(2):
        cols = slice(h * proj_half, (h + 1) * proj_half)
        stream = residual[:, cols].astype(f32) + (
            proj[0, h].astype(f32) + proj_sum[0, h].astype(f32) + proj_sum[1, h].astype(f32)
        )
        hidden[:, cols] = stream
        squares = squares + jnp.sum(stream * stream, axis=1, keepdims=True)
    scale_row = lax.rsqrt(squares * (1.0 / model_width) + norm_eps)
    for q in range(QUARTERS):
        cols = slice(q * width, (q + 1) * width)
        parted[q * rows_dev : (q + 1) * rows_dev] = (
            hidden[:, cols] * scale_row * gain[:, cols]
        ).astype(bf16)
    step_experts = experts // 4

    @pl.loop(0, 4)
    def _(n):
        first = pl.multiple_of(n * step_rows, step_rows)
        taken = jnp.dot(
            chosen[pl.ds(first, step_rows)], parted[...], preferred_element_type=f32
        ).astype(bf16)
        send[pl.ds(n * step_experts, step_experts)] = taken.reshape(
            step_experts, QUARTERS * capacity, width
        )

    half = chips // 2
    groups = half
    last = groups - 1
    block_rows = send.shape[1]
    rows = 4 * capacity
    half_model = QUARTERS * width // 2
    hidden_width = gate.shape[1]

    def remote(src, dst, send_sem, recv_sem, to):
        return pltpu.make_async_remote_copy(
            src_ref=src,
            dst_ref=dst,
            send_sem=send_sem,
            recv_sem=recv_sem,
            device_id=to,
            device_id_type=MESH,
        )

    def at_z(zt, ct):
        return {"sp_0": zt, "sp_1": ct}

    def chip_at(offset):
        return lax.rem(z + offset + chips, chips)

    def partner_out():
        return remote(
            send.at[z * CORES + 1 - c], gbuf.at[0, last, c], zs.at[4 * last], zr.at[4 * last],
            at_z(z, 1 - c),
        )

    def far_out(ct):
        zt = chip_at(half)
        return remote(
            send.at[zt * CORES + ct],
            gbuf.at[0, last, 2 + c],
            zs.at[4 * last + 2 + ct],
            zr.at[4 * last + 2 + c],
            at_z(zt, ct),
        )

    def near_out(d, sign, ct):
        zt = chip_at(d) if sign == 0 else chip_at(-d)
        return remote(
            send.at[zt * CORES + ct],
            gbuf.at[0, d - 1, 2 * sign + c],
            zs.at[4 * (d - 1) + 2 * sign + ct],
            zr.at[4 * (d - 1) + 2 * sign + c],
            at_z(zt, ct),
        )

    partner_out().start()

    @pl.loop(1, half)
    def _(d):
        for ct in range(CORES):
            for sign in range(2):
                near_out(d, sign, ct).start()

    for ct in range(CORES):
        far_out(ct).start()
    gbuf[0, last, c] = send[me]
    for load in loads[9:]:
        load.wait()

    def z_arrived(g, j):
        return remote(send.at[0], gbuf.at[0, g, j], zs.at[0], zr.at[4 * g + j], at_z(z, 1 - c))

    def spread(side, g):
        return remote(
            gbuf.at[0, g],
            gbuf.at[1 + side, g],
            xs.at[side, g],
            xr.at[side, g],
            at_x(right if side == 0 else left),
        )

    def relay(side, g):
        return remote(
            gbuf.at[1 + side, g, pl.ds(2 * side, 2)],
            gbuf.at[3, g, pl.ds(2 * side, 2)],
            ys.at[side, g],
            yr.at[side, g],
            at_x(right if side == 0 else left),
        )

    def stage_a(g):
        @pl.when(g < last)
        def _():
            for j in range(4):
                z_arrived(g, j).wait_recv()

        @pl.when(g == last)
        def _():
            for j in (0, 2, 3):
                z_arrived(g, j).wait_recv()

        for side in range(2):
            spread(side, g).start()

    def stage_b(g):
        for side in range(2):
            spread(side, g).wait_recv()
            relay(side, g).start()

    def far_half(side, g):
        return remote(
            pbuf.at[g, 3, side],
            rbuf.at[side, g],
            ds.at[side, g],
            dr.at[side, g],
            at_x(right if side == 0 else left),
        )

    def plain_half(side, g):
        return remote(
            pbuf.at[g, 2 - side, 1 - side],
            sbuf.at[side, 1 - side, g],
            es.at[side, 0, g],
            er.at[side, 0, g],
            at_x(right if side == 0 else left),
        )

    def added_half(side, g):
        return remote(
            pbuf.at[g, 2 - side, side],
            sbuf.at[side, side, g],
            es.at[side, 1, g],
            er.at[side, 1, g],
            at_x(right if side == 0 else left),
        )

    def stage_c(g):
        for side in range(2):
            relay(side, g).wait_recv()
        for part in range(4):
            block = gbuf[part, g].reshape(4 * block_rows, width)
            turned = jnp.dot(perm[...], block, preferred_element_type=jnp.float32).astype(
                jnp.bfloat16
            )
            for q in range(QUARTERS):
                xbuf[pl.ds(part * rows, rows), pl.ds(q * width, width)] = turned[
                    q * rows : (q + 1) * rows
                ]
        step = min(256, hidden_width)

        @pl.loop(0, hidden_width // step)
        def _(n):
            cols = pl.ds(pl.multiple_of(n * step, step), step)
            gate_pre = jnp.dot(xbuf[...], gate[:, cols], preferred_element_type=jnp.float32)
            up_pre = jnp.dot(xbuf[...], up[:, cols], preferred_element_type=jnp.float32)
            hbuf[:, cols] = activate(gate_pre, up_pre).astype(jnp.bfloat16)

        out_step = min(512, half_model)

        @pl.loop(0, half_model // out_step)
        def _(n):
            for side in range(2):
                cols = pl.ds(
                    pl.multiple_of(side * half_model + n * out_step, out_step), out_step
                )
                here = pl.ds(pl.multiple_of(n * out_step, out_step), out_step)
                part_sum = jnp.dot(
                    hbuf[...], down[:, cols], preferred_element_type=jnp.float32
                ).astype(jnp.bfloat16)
                for part in range(4):
                    pbuf[g, part, side, :, here] = part_sum[part * rows : (part + 1) * rows]

        for side in range(2):
            far_half(side, g).start()
        for side in range(2):
            plain_half(side, g).start()

    def stage_e(g):
        for side in range(2):
            far_half(side, g).wait_recv()
            pbuf[g, 2 - side, side] = (
                pbuf[g, 2 - side, side].astype(jnp.float32) + rbuf[side, g].astype(jnp.float32)
            ).astype(jnp.bfloat16)
            added_half(side, g).start()

    def stage_f(g):
        for side in range(2):
            plain_half(side, g).wait_recv()
            added_half(side, g).wait_recv()
        quarters = []
        for h in range(2):
            total = (
                pbuf[g, 0, h].astype(jnp.float32)
                + sbuf[0, h, g].astype(jnp.float32)
                + sbuf[1, h, g].astype(jnp.float32)
            ).astype(jnp.bfloat16)
            quarters += [total[:, :width], total[:, width:]]
        stacked = jnp.concatenate(quarters, axis=0)
        ret[g] = (
            jnp.dot(perm_back[...], stacked, preferred_element_type=jnp.float32)
            .astype(jnp.bfloat16)
            .reshape(4, block_rows, width)
        )

    def near_back(g, sign, cs):
        zt = chip_at(-g - 1) if sign == 0 else chip_at(g + 1)
        return remote(
            ret.at[g, 2 * sign + cs],
            back.at[me],
            rs.at[4 * g + 2 * sign + cs],
            rr.at[4 * g + 2 * sign + c],
            at_z(zt, cs),
        )

    def far_back(cs):
        return remote(
            ret.at[last, 2 + cs],
            back.at[me],
            rs.at[4 * last + 2 + cs],
            rr.at[4 * last + 2 + c],
            at_z(chip_at(half), cs),
        )

    def partner_back():
        return remote(
            ret.at[last, 1 - c], back.at[me], rs.at[4 * last], rr.at[4 * last], at_z(z, 1 - c)
        )

    def stage_h(g):
        @pl.when(g < last)
        def _():
            for cs in range(CORES):
                for sign in range(2):
                    near_back(g, sign, cs).start()

        @pl.when(g == last)
        def _():
            for cs in range(CORES):
                far_back(cs).start()
            partner_back().start()
            back[me] = ret[last, c]

    @pl.loop(0, groups + 4)
    def _(i):
        @pl.when(i >= 4)
        def _():
            stage_f(i - 4)

        @pl.when(i >= 4)
        def _():
            stage_h(i - 4)

        @pl.when((i >= 3) & (i < groups + 3))
        def _():
            stage_e(i - 3)

        @pl.when((i >= 2) & (i < groups + 2))
        def _():
            stage_c(i - 2)

        @pl.when((i >= 1) & (i < groups + 1))
        def _():
            stage_b(i - 1)

        @pl.when(i < groups)
        def _():
            stage_a(i)

    partner_out().wait_send()
    partner_back().wait_send()
    partner_back().wait_recv()
    for ct in range(CORES):
        far_out(ct).wait_send()
        far_back(ct).wait_send()

    def back_arrived(g, j):
        return remote(ret.at[0, 0], back.at[0], rs.at[0], rr.at[4 * g + j], at_z(z, 1 - c))

    for j in (2, 3):
        back_arrived(last, j).wait_recv()

    @pl.loop(0, last)
    def _(g):
        for sign in range(2):
            for ct in range(CORES):
                near_out(g + 1, sign, ct).wait_send()
                near_back(g, sign, ct).wait_send()
        for j in range(4):
            back_arrived(g, j).wait_recv()

    @pl.loop(0, groups)
    def _(g):
        for side in range(2):
            spread(side, g).wait_send()
            relay(side, g).wait_send()
            far_half(side, g).wait_send()
            plain_half(side, g).wait_send()
            added_half(side, g).wait_send()

    arrived_rows = back[...].reshape(slots, width)
    for q in range(QUARTERS):
        own = slice(q * rows_dev, (q + 1) * rows_dev)
        cols = slice(q * width, (q + 1) * width)
        total = hidden[:, cols]
        for k in range(TOP_K):
            total = total + route_weights[:, k : k + 1] * jnp.dot(
                picks[k, own], arrived_rows, preferred_element_type=f32
            )
        out[:, cols] = total.astype(bf16)

    @pl.loop(1, devices)
    def _(step):
        piece_out(step).wait_send()
        answer_out(step).wait_send()

    for side in range(2):
        proj_far_half(side).wait_send()
        proj_plain_half(side).wait_send()
        proj_added_half(side).wait_send()


def layer_stage(
    query_wide,
    key_wide,
    value_wide,
    decay_wide,
    query_narrow,
    key_narrow,
    value_narrow,
    decay_narrow,
    residual,
    out_wide,
    out_narrow,
    norm_gain,
    routes,
    route_weights,
    gate,
    up,
    down,
):
    length = query_wide.shape[0]
    chips = lax.axis_size("sp_0")
    devices = chips * CORES
    groups = chips // 2
    rows_dev, model_width = residual.shape
    width = model_width // QUARTERS
    hidden_width = gate.shape[1]
    capacity = max(2, 3 * rows_dev * TOP_K // (2 * devices))
    block_rows = QUARTERS * capacity
    rows = 4 * capacity
    slots = devices * block_rows
    table = regroup(capacity)
    decay = jnp.concatenate(
        [decay_wide, decay_narrow, jnp.zeros((length, 2), jnp.float32)], axis=1
    )
    positions = (lax.axis_index(SP) * length + jnp.arange(length, dtype=jnp.int32)).astype(
        jnp.float32
    )
    inverse = [
        rotary_base ** (-jnp.arange(size // 2, dtype=jnp.float32) / (size // 2))
        for size in (HEAD_WIDE, HEAD_NARROW)
    ]
    inverse = jnp.concatenate(inverse + [jnp.zeros((HEAD_NARROW // 2,), jnp.float32)])
    angles = positions[:, None] * inverse[None, :]
    turns = jnp.concatenate([jnp.cos(angles), jnp.sin(angles)], axis=1)
    vmem = pl.BlockSpec(memory_space=pltpu.VMEM)
    hbm = pl.BlockSpec(memory_space=pl.ANY)
    bf16 = jnp.bfloat16
    f32 = jnp.float32
    dma = pltpu.SemaphoreType.DMA
    piece_rows = 2 * HEAD_WIDE // devices
    moved = pltpu.VMEM((devices, piece_rows, 2 * HEAD_WIDE), bf16)
    heads = pltpu.VMEM(query_wide.shape, bf16)
    half = model_width // 2
    from_hbm = (
        query_wide,
        key_wide,
        value_wide,
        query_narrow,
        key_narrow,
        value_narrow,
        out_wide,
        out_narrow,
        residual,
        gate,
        up,
        down,
    )
    return pl.pallas_call(
        functools.partial(layer_kernel, chips),
        out_shape=jax.ShapeDtypeStruct(residual.shape, bf16),
        in_specs=[vmem] * 8 + [hbm] * 12,
        out_specs=vmem,
        scratch_shapes=[pltpu.VMEM(a.shape, bf16) for a in from_hbm]
        + [
            pltpu.VMEM((rows_dev, model_width), f32),
            pltpu.VMEM((QUARTERS * rows_dev, width), bf16),
            pltpu.VMEM((slots, QUARTERS * rows_dev), bf16),
            pltpu.VMEM((TOP_K, QUARTERS * rows_dev, slots), bf16),
            pltpu.VMEM((devices, block_rows, width), bf16),
            pltpu.VMEM((devices, block_rows, width), bf16),
            pltpu.VMEM((4, length, HEAD_WIDE), bf16),
            pltpu.VMEM((4, length, HEAD_WIDE), bf16),
            pltpu.VMEM((4, length, HEAD_WIDE), f32),
            pltpu.VMEM((length, 4 * HEAD_WIDE), bf16),
            moved,
            moved,
            moved,
            moved,
            pltpu.VMEM((4, 2, rows_dev, half), bf16),
            pltpu.VMEM((2, rows_dev, half), bf16),
            pltpu.VMEM((2, 2, rows_dev, half), bf16),
            pltpu.VMEM((4, groups, 4, block_rows, width), bf16),
            pltpu.VMEM((4 * rows, model_width), bf16),
            pltpu.VMEM((4 * rows, hidden_width), bf16),
            pltpu.VMEM((groups, 4, 2, rows, half), bf16),
            pltpu.VMEM((2, groups, rows, half), bf16),
            pltpu.VMEM((2, 2, groups, rows, half), bf16),
            pltpu.VMEM((groups, 4, block_rows, width), bf16),
            dma((12,)),
            dma((devices,)),
            dma((devices,)),
            dma((devices,)),
            dma((devices,)),
            dma((2,)),
            dma((2,)),
            dma((2, 2)),
            dma((2, 2)),
            dma((4 * groups,)),
            dma((4 * groups,)),
            dma((2, groups)),
            dma((2, groups)),
            dma((2, groups)),
            dma((2, groups)),
            dma((2, groups)),
            dma((2, groups)),
            dma((2, 2, groups)),
            dma((2, 2, groups)),
            dma((4 * groups,)),
            dma((4 * groups,)),
        ],
        compiler_params=pltpu.CompilerParams(
            collective_id=0, has_side_effects=True, vmem_limit_bytes=60 * 1024 * 1024
        ),
        name="layer_stage",
    )(
        decay,
        decay.T,
        turns,
        norm_gain[None, :],
        routes,
        route_weights,
        jnp.asarray(table, bf16),
        jnp.asarray(table.T, bf16),
        *from_hbm,
    )


def body(*arguments):
    return layer_stage(*arguments[:14], *(weight[0] for weight in arguments[14:]))


def solution(mesh):
    torus = Mesh(
        mesh.devices.reshape(mesh.shape["grp"], 16, 2, mesh.shape["tp"]),
        ("grp", "sp_0", "sp_1", "tp"),
    )
    in_specs = (
        P(GRP_SP, "tp"),
        P(GRP_SP, "tp"),
        P(GRP_SP, "tp"),
        P(GRP_SP, "tp"),
        P(GRP_SP, "tp"),
        P(GRP_SP, "tp"),
        P(GRP_SP, "tp"),
        P(GRP_SP, "tp"),
        P(GRP_SP_TP, None),
        P("tp", None),
        P("tp", None),
        P(),
        P(GRP_SP_TP, None),
        P(GRP_SP_TP, None),
        P(SP, None, "tp"),
        P(SP, None, "tp"),
        P(SP, "tp", None),
    )
    out_specs = P(GRP_SP_TP, None)
    return jax.shard_map(body, mesh=torus, in_specs=in_specs, out_specs=out_specs, check_vma=False)
```

```python
import functools

import jax
import jax.numpy as jnp
import numpy as np
from jax import lax
from jax.experimental import pallas as pl
from jax.experimental.pallas import tpu as pltpu
from jax.sharding import Mesh
from jax.sharding import PartitionSpec as P

HEAD_WIDE = 128
HEAD_NARROW = 64
TOP_K = 2
SP = ("sp_0", "sp_1")
GRP_SP = ("grp", "sp_0", "sp_1")
GRP_SP_TP = ("grp", "sp_0", "sp_1", "tp")


norm_eps = 1e-05
clamp_limit = 7.0
swish_alpha = 1.702
rotary_base = 10000.0


def activate(gate_pre, up_pre):
    gate_clip = jnp.minimum(gate_pre, clamp_limit)
    up_clip = jnp.clip(up_pre, -clamp_limit, clamp_limit)
    return gate_clip * jax.nn.sigmoid(swish_alpha * gate_clip) * (up_clip + 1.0)


QUARTERS = 4
CORES = 2
MESH = pl.DeviceIdType.MESH


def regroup(capacity):
    rows = 4 * QUARTERS * capacity
    table = np.zeros((rows, rows), np.float32)
    for block in range(4):
        for part in range(QUARTERS):
            for row in range(capacity):
                table[
                    (part * 4 + block) * capacity + row, (block * QUARTERS + part) * capacity + row
                ] = 1.0
    return table


def in_three(value):
    first = value.astype(jnp.bfloat16)
    rest = value - first.astype(jnp.float32)
    second = rest.astype(jnp.bfloat16)
    third = (rest - second.astype(jnp.float32)).astype(jnp.bfloat16)
    return (first, second, third)


def lanes_of(shape):
    return lax.broadcasted_iota(jnp.int32, shape, len(shape) - 1)


def rows_of(shape):
    return lax.broadcasted_iota(jnp.int32, shape, 0)


def dot_f32(a, b, contract):
    return lax.dot_general(a, b, (contract, ((), ())), preferred_element_type=jnp.float32)


def layer_kernel(
    chips,
    decay_wide,
    decay_narrow,
    near_hbm,
    block_turns,
    gain,
    routes,
    route_weights,
    perm,
    perm_back,
    query_wide_hbm,
    key_wide_hbm,
    value_wide_hbm,
    query_narrow_hbm,
    key_narrow_hbm,
    value_narrow_hbm,
    out_wide_hbm,
    out_narrow_hbm,
    residual_hbm,
    gate_hbm,
    up_hbm,
    down_hbm,
    out,
    query_wide,
    key_wide,
    value_wide,
    query_narrow,
    key_narrow,
    value_narrow,
    out_wide,
    out_narrow,
    residual,
    gate,
    up,
    down,
    near,
    hidden,
    parted,
    chosen,
    picks,
    send,
    back,
    qbuf,
    kbuf,
    inner,
    mixed,
    pieces,
    arrived,
    answers,
    states,
    proj,
    proj_far,
    proj_sum,
    gbuf,
    xbuf,
    hbuf,
    pbuf,
    rbuf,
    sbuf,
    ret,
    load_sem,
    p1s,
    p1r,
    p2s,
    p2r,
    pds,
    pdr,
    pes,
    per,
    zs,
    zr,
    xs,
    xr,
    ys,
    yr,
    ds,
    dr,
    es,
    er,
    rs,
    rr,
):
    z = lax.axis_index("sp_0")
    c = lax.axis_index("sp_1")
    x = lax.axis_index("tp")
    nx = lax.axis_size("tp")
    devices = chips * CORES
    me = z * CORES + c
    right = lax.rem(x + 1, nx)
    left = lax.rem(x + nx - 1, nx)
    length = query_wide.shape[0]
    units = 4
    lane = HEAD_WIDE
    block = min(128, length)
    f32 = jnp.float32
    bf16 = jnp.bfloat16

    def peer(step):
        other = lax.rem(me + step, devices)
        return other, {"sp_0": other // CORES, "sp_1": lax.rem(other, CORES)}

    def at_x(xt):
        return {"tp": xt}

    loads = [
        pltpu.make_async_copy(source, target, load_sem.at[n])
        for n, (source, target) in enumerate(
            (
                (near_hbm, near),
                (key_wide_hbm, key_wide),
                (key_narrow_hbm, key_narrow),
                (value_wide_hbm, value_wide),
                (value_narrow_hbm, value_narrow),
                (query_wide_hbm, query_wide),
                (query_narrow_hbm, query_narrow),
                (out_wide_hbm, out_wide),
                (out_narrow_hbm, out_narrow),
                (residual_hbm, residual),
                (gate_hbm, gate),
                (up_hbm, up),
                (down_hbm, down),
            )
        )
    ]
    for load in loads[:7]:
        load.start()

    barrier = pltpu.get_barrier_semaphore()
    pl.semaphore_signal(barrier, inc=1, device_id=at_x(right), device_id_type=MESH)
    pl.semaphore_signal(barrier, inc=1, device_id=at_x(left), device_id_type=MESH)

    @pl.loop(1, devices)
    def _(step):
        pl.semaphore_signal(barrier, inc=1, device_id=peer(step)[1], device_id_type=MESH)

    for load in loads[7:]:
        load.start()

    square = (length, length)
    below = (rows_of(square) >= lanes_of(square)).astype(f32).astype(bf16)
    decay_t = jnp.concatenate(
        [decay_wide[...], decay_narrow[...], jnp.zeros((2, length), f32)], axis=0
    )
    terms = in_three(decay_t)
    cum = sum(dot_f32(below, term, ((1,), (1,))) for term in terms)
    cum_t = sum(dot_f32(term, below, ((1,), (1,))) for term in terms)

    table_lane = lanes_of((length, lane))
    loads[0].wait()
    start = block_turns[me]
    start_cos = start[:, :lane]
    start_sin = start[:, lane:]
    cos_all = near[:, :lane] * start_cos - near[:, lane:] * start_sin
    sin_all = near[:, lane:] * start_cos + near[:, :lane] * start_sin
    low = table_lane < HEAD_WIDE // 2

    def wide_table(table):
        return jnp.where(low, table, pltpu.roll(table, HEAD_WIDE // 2, 1))

    def narrow_table(table):
        first = pltpu.roll(table, 64, 1)
        twice = jnp.where(table_lane < 32, first, pltpu.roll(first, 32, 1))
        return jnp.where(low, twice, pltpu.roll(twice, 64, 1))

    wide_cos = wide_table(cos_all)
    wide_sin = wide_table(sin_all)
    wide_sin = jnp.where(low, -wide_sin, wide_sin)
    narrow_cos = narrow_table(cos_all)
    narrow_sin = narrow_table(sin_all)
    narrow_low = lax.rem(table_lane, HEAD_NARROW) < HEAD_NARROW // 2
    narrow_sin = jnp.where(narrow_low, -narrow_sin, narrow_sin)

    def turned(source, unit):
        wide = unit < 2
        lanes = slice((unit % 2) * lane, (unit % 2 + 1) * lane)
        values = source[:, lanes].astype(f32)
        if wide:
            return values * wide_cos + pltpu.roll(values, HEAD_WIDE // 2, 1) * wide_sin
        swapped = jnp.where(
            narrow_low,
            pltpu.roll(values, lane - HEAD_NARROW // 2, 1),
            pltpu.roll(values, HEAD_NARROW // 2, 1),
        )
        return values * narrow_cos + swapped * narrow_sin

    def values_of(unit):
        source = value_wide if unit < 2 else value_narrow
        return source[:, (unit % 2) * lane : (unit % 2 + 1) * lane]

    def heads_of(unit):
        return (unit,) if unit < 2 else (2 * unit - 2, 2 * unit - 1)

    def per_lane(unit, column):
        heads = heads_of(unit)
        if len(heads) == 1:
            return column(heads[0])
        shape = (column(heads[0]).shape[0], lane)
        return jnp.where(lanes_of(shape) < HEAD_NARROW, column(heads[0]), column(heads[1]))

    def total_of(head):
        return cum_t[head : head + 1, length - 1 : length]

    unit_shape = (lane, lane)
    unit_low_row = rows_of(unit_shape) < HEAD_NARROW
    unit_low_lane = lanes_of(unit_shape) < HEAD_NARROW
    for load in loads[1:5]:
        load.wait()
    local = []
    for unit in range(units):
        width = HEAD_WIDE if unit < 2 else HEAD_NARROW
        key = (turned(key_wide if unit < 2 else key_narrow, unit) * width ** (-0.5)).astype(bf16)
        kbuf[unit] = key
        weight = per_lane(unit, lambda h: jnp.exp(total_of(h) - cum[:, h : h + 1]))
        weighted = (key.astype(f32) * weight).astype(bf16)
        state = dot_f32(weighted, values_of(unit), ((0,), (0,)))
        if unit < 2:
            local.append(state)
        else:
            packed = jnp.where(unit_low_row, state, pltpu.roll(state, HEAD_NARROW, 1))
            wide_total = total_of(unit - 2)
            narrow_total = jnp.where(
                unit_low_row, total_of(heads_of(unit)[0]), total_of(heads_of(unit)[1])
            )
            lane_id = lanes_of(unit_shape)
            for position, term in enumerate(
                in_three(jnp.broadcast_to(wide_total, unit_shape)) + in_three(narrow_total)
            ):
                packed = jnp.where(
                    lane_id == HEAD_NARROW + position, term.astype(f32), packed
                )
            local.append(packed)
    piece_rows = 2 * lane // devices
    for unit in range(units):
        here = slice((unit % 2) * (devices // 2), (unit % 2 + 1) * (devices // 2))
        lanes = slice((unit // 2) * lane, (unit // 2 + 1) * lane)
        pieces[here, :, lanes] = local[unit].reshape(devices // 2, piece_rows, lane).astype(bf16)

    pl.semaphore_wait(barrier, 2 + devices - 1)

    def piece_out(step):
        other, where = peer(step)
        return pltpu.make_async_remote_copy(
            src_ref=pieces.at[other],
            dst_ref=arrived.at[me],
            send_sem=p1s.at[step],
            recv_sem=p1r.at[step],
            device_id=where,
            device_id_type=MESH,
        )

    def answer_out(step):
        other, where = peer(step)
        return pltpu.make_async_remote_copy(
            src_ref=answers.at[other],
            dst_ref=states.at[me],
            send_sem=p2s.at[step],
            recv_sem=p2r.at[step],
            device_id=where,
            device_id_type=MESH,
        )

    @pl.loop(1, devices)
    def _(step):
        piece_out(step).start()

    arrived[me] = pieces[me]

    for load in loads[5:7]:
        load.wait()
    for unit in range(units):
        qbuf[unit] = turned(query_wide if unit < 2 else query_narrow, unit).astype(bf16)

    def within(unit):
        for start in range(0, length, block):
            stop = start + block
            shape = (block, stop)
            causal = rows_of(shape) + start >= lanes_of(shape)
            query = qbuf[unit, start:stop]
            key = kbuf[unit, :stop]
            value = values_of(unit)[:stop]
            outs = []
            for n, head in enumerate(heads_of(unit)):
                own = query
                if unit >= 2:
                    mine = lax.div(lanes_of((block, lane)), HEAD_NARROW) == n
                    own = jnp.where(mine, query.astype(f32), 0.0).astype(bf16)
                scores = dot_f32(own, key, ((1,), (1,)))
                gaps = cum[start:stop, head : head + 1] - cum_t[head : head + 1, :stop]
                faded = scores * jnp.exp(jnp.where(causal, gaps, -jnp.inf))
                outs.append(dot_f32(faded.astype(bf16), value, ((1,), (0,))))
            if unit >= 2:
                outs = [jnp.where(lanes_of((block, lane)) < HEAD_NARROW, outs[0], outs[1])]
            inner[unit, start:stop] = outs[0]

    for unit in range(2):
        within(unit)

    @pl.loop(1, devices)
    def _(step):
        piece_out(step).wait_recv()

    running = jnp.zeros((piece_rows, 2 * lane), f32)
    piece_lane = lanes_of((piece_rows, lane))
    for source in range(devices):
        answers[source] = running.astype(bf16)
        came = arrived[source].astype(f32)
        tail = came[:, lane:]

        def log_at(first):
            terms = (piece_lane >= first) & (piece_lane < first + 3)
            return jnp.sum(jnp.where(terms, tail, 0.0), axis=1, keepdims=True)

        scale = jnp.concatenate(
            [
                jnp.broadcast_to(jnp.exp(log_at(HEAD_NARROW)), piece_lane.shape),
                jnp.broadcast_to(jnp.exp(log_at(HEAD_NARROW + 3)), piece_lane.shape),
            ],
            axis=1,
        )
        running = scale * running + came

    @pl.loop(1, devices)
    def _(step):
        answer_out(step).start()

    states[me] = answers[me]

    for unit in range(2, units):
        within(unit)

    @pl.loop(1, devices)
    def _(step):
        answer_out(step).wait_recv()

    for unit in range(units):
        here = slice((unit % 2) * (devices // 2), (unit % 2 + 1) * (devices // 2))
        lanes = slice((unit // 2) * lane, (unit // 2 + 1) * lane)
        state = states[here, :, lanes].astype(f32).reshape(lane, lane)
        if unit >= 2:
            state = jnp.where(
                unit_low_row,
                jnp.where(unit_low_lane, state, 0.0),
                jnp.where(unit_low_lane, 0.0, pltpu.roll(state, HEAD_NARROW, 1)),
            )
        carried = dot_f32(qbuf[unit], state.astype(bf16), ((1,), (0,)))
        kept = per_lane(unit, lambda h: jnp.exp(cum[:, h : h + 1]))
        value = inner[unit] + kept * carried

        def mean_of(entries):
            if unit < 2:
                return jnp.mean(entries, axis=1, keepdims=True)
            first = jnp.sum(jnp.where(low, entries, 0.0), axis=1, keepdims=True)
            second = jnp.sum(jnp.where(low, 0.0, entries), axis=1, keepdims=True)
            return jnp.where(low, first, second) * (1.0 / HEAD_NARROW)

        centered = value - mean_of(value)
        spread = mean_of(centered * centered)
        mixed[:, unit * lane : (unit + 1) * lane] = (
            centered * lax.rsqrt(spread + norm_eps)
        ).astype(bf16)

    rows_dev = length // nx
    model_width = out_wide.shape[1]
    proj_half = model_width // 2

    for load in loads[7:10]:
        load.wait()

    def x_copy(src, dst, send_sem, recv_sem, side):
        return pltpu.make_async_remote_copy(
            src_ref=src,
            dst_ref=dst,
            send_sem=send_sem,
            recv_sem=recv_sem,
            device_id=at_x(right if side == 0 else left),
            device_id_type=MESH,
        )

    def proj_far_half(side):
        return x_copy(proj.at[3, side], proj_far.at[side], pds.at[side], pdr.at[side], side)

    def proj_plain_half(side):
        return x_copy(
            proj.at[2 - side, 1 - side], proj_sum.at[side, 1 - side], pes.at[side, 0], per.at[side, 0], side
        )

    def proj_added_half(side):
        return x_copy(
            proj.at[2 - side, side], proj_sum.at[side, side], pes.at[side, 1], per.at[side, 1], side
        )

    out_step = min(512, proj_half)

    def project(part, side):
        target = (x, left, right, lax.rem(x + 2, nx))[part]
        own_rows = pl.ds(pl.multiple_of(target * rows_dev, rows_dev), rows_dev)

        @pl.loop(0, proj_half // out_step)
        def _(n):
            cols = pl.ds(pl.multiple_of(side * proj_half + n * out_step, out_step), out_step)
            here = pl.ds(pl.multiple_of(n * out_step, out_step), out_step)
            both = jnp.dot(
                mixed[own_rows, : 2 * lane], out_wide[:, cols], preferred_element_type=f32
            ) + jnp.dot(
                mixed[own_rows, 2 * lane :], out_narrow[:, cols], preferred_element_type=f32
            )
            proj[part, side, :, here] = both.astype(bf16)

    for side in range(2):
        project(3, side)
        proj_far_half(side).start()
    for side in range(2):
        project(2 - side, 1 - side)
        proj_plain_half(side).start()
    for side in range(2):
        project(2 - side, side)
    for side in range(2):
        project(0, side)
    for side in range(2):
        proj_far_half(side).wait_recv()
        proj[2 - side, side] = (
            proj[2 - side, side].astype(f32) + proj_far[side].astype(f32)
        ).astype(bf16)
        proj_added_half(side).start()
    experts = devices
    one_hots = []
    for k in range(TOP_K):
        wanted = jnp.broadcast_to(routes[k : k + 1, :], (experts, rows_dev))
        one_hots.append((wanted == rows_of((experts, rows_dev))).astype(f32))
    rows_square = (rows_dev, rows_dev)
    earlier = (rows_of(rows_square) < lanes_of(rows_square)).astype(f32).astype(bf16)
    diagonal = rows_of(rows_square) == lanes_of(rows_square)

    def stood_up(row):
        return jnp.sum(
            jnp.where(diagonal, jnp.broadcast_to(row, rows_square), 0.0), axis=1, keepdims=True
        )

    before = jnp.zeros((experts, 1), f32)
    parts = QUARTERS * rows_dev
    slots = send.shape[0] * send.shape[1]
    capacity = send.shape[1] // QUARTERS
    width = send.shape[2]
    picked_rows = []
    for k in range(TOP_K):
        ahead = dot_f32(one_hots[k].astype(bf16), earlier, ((1,), (0,))) + before
        rank = jnp.sum(ahead * one_hots[k], axis=0, keepdims=True)
        before = before + jnp.sum(one_hots[k], axis=1, keepdims=True)
        across = routes[k : k + 1, :].astype(f32) * float(QUARTERS * capacity) + rank
        place = stood_up(across)
        picked_rows.append(
            jnp.concatenate([across + float(q * capacity) for q in range(QUARTERS)], axis=1)
        )
        for q in range(QUARTERS):
            own = slice(q * rows_dev, (q + 1) * rows_dev)
            wanted = jnp.broadcast_to(place + float(q * capacity), (rows_dev, slots))
            picks[k, own] = (
                (wanted == lanes_of((rows_dev, slots)).astype(f32)).astype(f32).astype(bf16)
            )
    step_rows = slots // 4

    @pl.loop(0, 4)
    def _(n):
        first = pl.multiple_of(n * step_rows, step_rows)
        slot = (rows_of((step_rows, parts)) + first).astype(f32)
        hit = (slot == picked_rows[0]) | (slot == picked_rows[1])
        chosen[pl.ds(first, step_rows)] = hit.astype(f32).astype(bf16)

    for side in range(2):
        proj_plain_half(side).wait_recv()
        proj_added_half(side).wait_recv()
    squares = jnp.zeros((rows_dev, 1), f32)
    for h in range(2):
        cols = slice(h * proj_half, (h + 1) * proj_half)
        stream = residual[:, cols].astype(f32) + (
            proj[0, h].astype(f32) + proj_sum[0, h].astype(f32) + proj_sum[1, h].astype(f32)
        )
        hidden[:, cols] = stream
        squares = squares + jnp.sum(stream * stream, axis=1, keepdims=True)
    scale_row = lax.rsqrt(squares * (1.0 / model_width) + norm_eps)
    for q in range(QUARTERS):
        cols = slice(q * width, (q + 1) * width)
        parted[q * rows_dev : (q + 1) * rows_dev] = (
            hidden[:, cols] * scale_row * gain[:, cols]
        ).astype(bf16)
    step_experts = experts // 4

    @pl.loop(0, 4)
    def _(n):
        first = pl.multiple_of(n * step_rows, step_rows)
        taken = jnp.dot(
            chosen[pl.ds(first, step_rows)], parted[...], preferred_element_type=f32
        ).astype(bf16)
        send[pl.ds(n * step_experts, step_experts)] = taken.reshape(
            step_experts, QUARTERS * capacity, width
        )

    half = chips // 2
    groups = half
    last = groups - 1
    block_rows = send.shape[1]
    rows = 4 * capacity
    half_model = QUARTERS * width // 2
    hidden_width = gate.shape[1]

    def remote(src, dst, send_sem, recv_sem, to):
        return pltpu.make_async_remote_copy(
            src_ref=src,
            dst_ref=dst,
            send_sem=send_sem,
            recv_sem=recv_sem,
            device_id=to,
            device_id_type=MESH,
        )

    def at_z(zt, ct):
        return {"sp_0": zt, "sp_1": ct}

    def chip_at(offset):
        return lax.rem(z + offset + chips, chips)

    def partner_out():
        return remote(
            send.at[z * CORES + 1 - c], gbuf.at[0, last, c], zs.at[4 * last], zr.at[4 * last],
            at_z(z, 1 - c),
        )

    def far_out(ct):
        zt = chip_at(half)
        return remote(
            send.at[zt * CORES + ct],
            gbuf.at[0, last, 2 + c],
            zs.at[4 * last + 2 + ct],
            zr.at[4 * last + 2 + c],
            at_z(zt, ct),
        )

    def near_out(d, sign, ct):
        zt = chip_at(d) if sign == 0 else chip_at(-d)
        return remote(
            send.at[zt * CORES + ct],
            gbuf.at[0, d - 1, 2 * sign + c],
            zs.at[4 * (d - 1) + 2 * sign + ct],
            zr.at[4 * (d - 1) + 2 * sign + c],
            at_z(zt, ct),
        )

    partner_out().start()

    @pl.loop(1, half)
    def _(d):
        for ct in range(CORES):
            for sign in range(2):
                near_out(d, sign, ct).start()

    for ct in range(CORES):
        far_out(ct).start()
    gbuf[0, last, c] = send[me]
    for load in loads[10:]:
        load.wait()

    def z_arrived(g, j):
        return remote(send.at[0], gbuf.at[0, g, j], zs.at[0], zr.at[4 * g + j], at_z(z, 1 - c))

    def spread(side, g):
        return remote(
            gbuf.at[0, g],
            gbuf.at[1 + side, g],
            xs.at[side, g],
            xr.at[side, g],
            at_x(right if side == 0 else left),
        )

    def relay(side, g):
        return remote(
            gbuf.at[1 + side, g, pl.ds(2 * side, 2)],
            gbuf.at[3, g, pl.ds(2 * side, 2)],
            ys.at[side, g],
            yr.at[side, g],
            at_x(right if side == 0 else left),
        )

    def stage_a(g):
        @pl.when(g < last)
        def _():
            for j in range(4):
                z_arrived(g, j).wait_recv()

        @pl.when(g == last)
        def _():
            for j in (0, 2, 3):
                z_arrived(g, j).wait_recv()

        for side in range(2):
            spread(side, g).start()

    def stage_b(g):
        for side in range(2):
            spread(side, g).wait_recv()
            relay(side, g).start()

    def far_half(side, g):
        return remote(
            pbuf.at[g, 3, side],
            rbuf.at[side, g],
            ds.at[side, g],
            dr.at[side, g],
            at_x(right if side == 0 else left),
        )

    def plain_half(side, g):
        return remote(
            pbuf.at[g, 2 - side, 1 - side],
            sbuf.at[side, 1 - side, g],
            es.at[side, 0, g],
            er.at[side, 0, g],
            at_x(right if side == 0 else left),
        )

    def added_half(side, g):
        return remote(
            pbuf.at[g, 2 - side, side],
            sbuf.at[side, side, g],
            es.at[side, 1, g],
            er.at[side, 1, g],
            at_x(right if side == 0 else left),
        )

    def stage_c(g):
        for side in range(2):
            relay(side, g).wait_recv()
        for part in range(4):
            block = gbuf[part, g].reshape(4 * block_rows, width)
            turned = jnp.dot(perm[...], block, preferred_element_type=jnp.float32).astype(
                jnp.bfloat16
            )
            for q in range(QUARTERS):
                xbuf[pl.ds(part * rows, rows), pl.ds(q * width, width)] = turned[
                    q * rows : (q + 1) * rows
                ]
        step = min(256, hidden_width)

        @pl.loop(0, hidden_width // step)
        def _(n):
            cols = pl.ds(pl.multiple_of(n * step, step), step)
            gate_pre = jnp.dot(xbuf[...], gate[:, cols], preferred_element_type=jnp.float32)
            up_pre = jnp.dot(xbuf[...], up[:, cols], preferred_element_type=jnp.float32)
            hbuf[:, cols] = activate(gate_pre, up_pre).astype(jnp.bfloat16)

        out_step = min(512, half_model)

        @pl.loop(0, half_model // out_step)
        def _(n):
            for side in range(2):
                cols = pl.ds(
                    pl.multiple_of(side * half_model + n * out_step, out_step), out_step
                )
                here = pl.ds(pl.multiple_of(n * out_step, out_step), out_step)
                part_sum = jnp.dot(
                    hbuf[...], down[:, cols], preferred_element_type=jnp.float32
                ).astype(jnp.bfloat16)
                for part in range(4):
                    pbuf[g, part, side, :, here] = part_sum[part * rows : (part + 1) * rows]

        for side in range(2):
            far_half(side, g).start()
        for side in range(2):
            plain_half(side, g).start()

    def stage_e(g):
        for side in range(2):
            far_half(side, g).wait_recv()
            pbuf[g, 2 - side, side] = (
                pbuf[g, 2 - side, side].astype(jnp.float32) + rbuf[side, g].astype(jnp.float32)
            ).astype(jnp.bfloat16)
            added_half(side, g).start()

    def stage_f(g):
        for side in range(2):
            plain_half(side, g).wait_recv()
            added_half(side, g).wait_recv()
        quarters = []
        for h in range(2):
            total = (
                pbuf[g, 0, h].astype(jnp.float32)
                + sbuf[0, h, g].astype(jnp.float32)
                + sbuf[1, h, g].astype(jnp.float32)
            ).astype(jnp.bfloat16)
            quarters += [total[:, :width], total[:, width:]]
        stacked = jnp.concatenate(quarters, axis=0)
        ret[g] = (
            jnp.dot(perm_back[...], stacked, preferred_element_type=jnp.float32)
            .astype(jnp.bfloat16)
            .reshape(4, block_rows, width)
        )

    def near_back(g, sign, cs):
        zt = chip_at(-g - 1) if sign == 0 else chip_at(g + 1)
        return remote(
            ret.at[g, 2 * sign + cs],
            back.at[me],
            rs.at[4 * g + 2 * sign + cs],
            rr.at[4 * g + 2 * sign + c],
            at_z(zt, cs),
        )

    def far_back(cs):
        return remote(
            ret.at[last, 2 + cs],
            back.at[me],
            rs.at[4 * last + 2 + cs],
            rr.at[4 * last + 2 + c],
            at_z(chip_at(half), cs),
        )

    def partner_back():
        return remote(
            ret.at[last, 1 - c], back.at[me], rs.at[4 * last], rr.at[4 * last], at_z(z, 1 - c)
        )

    def stage_h(g):
        @pl.when(g < last)
        def _():
            for cs in range(CORES):
                for sign in range(2):
                    near_back(g, sign, cs).start()

        @pl.when(g == last)
        def _():
            for cs in range(CORES):
                far_back(cs).start()
            partner_back().start()
            back[me] = ret[last, c]

    @pl.loop(0, groups + 4)
    def _(i):
        @pl.when(i >= 4)
        def _():
            stage_f(i - 4)

        @pl.when(i >= 4)
        def _():
            stage_h(i - 4)

        @pl.when((i >= 3) & (i < groups + 3))
        def _():
            stage_e(i - 3)

        @pl.when((i >= 2) & (i < groups + 2))
        def _():
            stage_c(i - 2)

        @pl.when((i >= 1) & (i < groups + 1))
        def _():
            stage_b(i - 1)

        @pl.when(i < groups)
        def _():
            stage_a(i)

    partner_out().wait_send()
    partner_back().wait_send()
    partner_back().wait_recv()
    for ct in range(CORES):
        far_out(ct).wait_send()
        far_back(ct).wait_send()

    def back_arrived(g, j):
        return remote(ret.at[0, 0], back.at[0], rs.at[0], rr.at[4 * g + j], at_z(z, 1 - c))

    for j in (2, 3):
        back_arrived(last, j).wait_recv()

    @pl.loop(0, last)
    def _(g):
        for sign in range(2):
            for ct in range(CORES):
                near_out(g + 1, sign, ct).wait_send()
                near_back(g, sign, ct).wait_send()
        for j in range(4):
            back_arrived(g, j).wait_recv()

    @pl.loop(0, groups)
    def _(g):
        for side in range(2):
            spread(side, g).wait_send()
            relay(side, g).wait_send()
            far_half(side, g).wait_send()
            plain_half(side, g).wait_send()
            added_half(side, g).wait_send()

    arrived_rows = back[...].reshape(slots, width)
    shares = [stood_up(route_weights[k : k + 1, :]) for k in range(TOP_K)]
    for q in range(QUARTERS):
        own = slice(q * rows_dev, (q + 1) * rows_dev)
        cols = slice(q * width, (q + 1) * width)
        total = hidden[:, cols]
        for k in range(TOP_K):
            total = total + shares[k] * jnp.dot(
                picks[k, own], arrived_rows, preferred_element_type=f32
            )
        out[:, cols] = total

    @pl.loop(1, devices)
    def _(step):
        piece_out(step).wait_send()
        answer_out(step).wait_send()

    for side in range(2):
        proj_far_half(side).wait_send()
        proj_plain_half(side).wait_send()
        proj_added_half(side).wait_send()


def turn_tables(length, blocks):
    inverse = [
        rotary_base ** (-np.arange(size // 2) / (size // 2)) for size in (HEAD_WIDE, HEAD_NARROW)
    ]
    inverse = np.concatenate(inverse + [np.zeros(HEAD_NARROW // 2)])

    def table(positions):
        angles = positions[:, None] * inverse[None, :]
        return jnp.asarray(
            np.concatenate([np.cos(angles), np.sin(angles)], axis=1), jnp.float32
        )

    return table(np.arange(length)), table(np.arange(blocks) * length)[:, None, :]


def layer_stage(
    query_wide,
    key_wide,
    value_wide,
    decay_wide,
    query_narrow,
    key_narrow,
    value_narrow,
    decay_narrow,
    residual,
    out_wide,
    out_narrow,
    norm_gain,
    routes,
    route_weights,
    gate,
    up,
    down,
):
    length = query_wide.shape[0]
    chips = lax.axis_size("sp_0")
    devices = chips * CORES
    groups = chips // 2
    rows_dev, model_width = residual.shape
    width = model_width // QUARTERS
    hidden_width = gate.shape[1]
    capacity = max(2, 3 * rows_dev * TOP_K // (2 * devices))
    block_rows = QUARTERS * capacity
    rows = 4 * capacity
    slots = devices * block_rows
    table = regroup(capacity)
    near, block_turns = turn_tables(length, devices)
    vmem = pl.BlockSpec(memory_space=pltpu.VMEM)
    hbm = pl.BlockSpec(memory_space=pl.ANY)
    bf16 = jnp.bfloat16
    f32 = jnp.float32
    dma = pltpu.SemaphoreType.DMA
    piece_rows = 2 * HEAD_WIDE // devices
    moved = pltpu.VMEM((devices, piece_rows, 2 * HEAD_WIDE), bf16)
    heads = pltpu.VMEM(query_wide.shape, bf16)
    half = model_width // 2
    from_hbm = (
        query_wide,
        key_wide,
        value_wide,
        query_narrow,
        key_narrow,
        value_narrow,
        out_wide,
        out_narrow,
        residual,
        gate,
        up,
        down,
    )
    return pl.pallas_call(
        functools.partial(layer_kernel, chips),
        out_shape=jax.ShapeDtypeStruct(residual.shape, f32),
        in_specs=[vmem] * 2 + [hbm] + [vmem] * 6 + [hbm] * 12,
        out_specs=vmem,
        scratch_shapes=[pltpu.VMEM(a.shape, bf16) for a in from_hbm]
        + [
            pltpu.VMEM(near.shape, f32),
            pltpu.VMEM((rows_dev, model_width), f32),
            pltpu.VMEM((QUARTERS * rows_dev, width), bf16),
            pltpu.VMEM((slots, QUARTERS * rows_dev), bf16),
            pltpu.VMEM((TOP_K, QUARTERS * rows_dev, slots), bf16),
            pltpu.VMEM((devices, block_rows, width), bf16),
            pltpu.VMEM((devices, block_rows, width), bf16),
            pltpu.VMEM((4, length, HEAD_WIDE), bf16),
            pltpu.VMEM((4, length, HEAD_WIDE), bf16),
            pltpu.VMEM((4, length, HEAD_WIDE), f32),
            pltpu.VMEM((length, 4 * HEAD_WIDE), bf16),
            moved,
            moved,
            moved,
            moved,
            pltpu.VMEM((4, 2, rows_dev, half), bf16),
            pltpu.VMEM((2, rows_dev, half), bf16),
            pltpu.VMEM((2, 2, rows_dev, half), bf16),
            pltpu.VMEM((4, groups, 4, block_rows, width), bf16),
            pltpu.VMEM((4 * rows, model_width), bf16),
            pltpu.VMEM((4 * rows, hidden_width), bf16),
            pltpu.VMEM((groups, 4, 2, rows, half), bf16),
            pltpu.VMEM((2, groups, rows, half), bf16),
            pltpu.VMEM((2, 2, groups, rows, half), bf16),
            pltpu.VMEM((groups, 4, block_rows, width), bf16),
            dma((13,)),
            dma((devices,)),
            dma((devices,)),
            dma((devices,)),
            dma((devices,)),
            dma((2,)),
            dma((2,)),
            dma((2, 2)),
            dma((2, 2)),
            dma((4 * groups,)),
            dma((4 * groups,)),
            dma((2, groups)),
            dma((2, groups)),
            dma((2, groups)),
            dma((2, groups)),
            dma((2, groups)),
            dma((2, groups)),
            dma((2, 2, groups)),
            dma((2, 2, groups)),
            dma((4 * groups,)),
            dma((4 * groups,)),
        ],
        compiler_params=pltpu.CompilerParams(
            collective_id=0, has_side_effects=True, vmem_limit_bytes=60 * 1024 * 1024
        ),
        name="layer_stage",
    )(
        decay_wide.T,
        decay_narrow.T,
        near,
        block_turns,
        norm_gain[None, :],
        routes.T,
        route_weights.T,
        jnp.asarray(table, bf16),
        jnp.asarray(table.T, bf16),
        *from_hbm,
    ).astype(bf16)


def body(*arguments):
    return layer_stage(*arguments[:14], *(weight[0] for weight in arguments[14:]))


def solution(mesh):
    torus = Mesh(
        mesh.devices.reshape(mesh.shape["grp"], 16, 2, mesh.shape["tp"]),
        ("grp", "sp_0", "sp_1", "tp"),
    )
    in_specs = (
        P(GRP_SP, "tp"),
        P(GRP_SP, "tp"),
        P(GRP_SP, "tp"),
        P(GRP_SP, "tp"),
        P(GRP_SP, "tp"),
        P(GRP_SP, "tp"),
        P(GRP_SP, "tp"),
        P(GRP_SP, "tp"),
        P(GRP_SP_TP, None),
        P("tp", None),
        P("tp", None),
        P(),
        P(GRP_SP_TP, None),
        P(GRP_SP_TP, None),
        P(SP, None, "tp"),
        P(SP, None, "tp"),
        P(SP, "tp", None),
    )
    out_specs = P(GRP_SP_TP, None)
    return jax.shard_map(body, mesh=torus, in_specs=in_specs, out_specs=out_specs, check_vma=False)
```

```python
import functools

import jax
import jax.numpy as jnp
import numpy as np
from jax import lax
from jax.experimental import pallas as pl
from jax.experimental.pallas import tpu as pltpu
from jax.sharding import Mesh
from jax.sharding import PartitionSpec as P

HEAD_WIDE = 128
HEAD_NARROW = 64
TOP_K = 2
SP = ("sp_0", "sp_1")
GRP_SP = ("grp", "sp_0", "sp_1")
GRP_SP_TP = ("grp", "sp_0", "sp_1", "tp")


norm_eps = 1e-05
clamp_limit = 7.0
swish_alpha = 1.702
rotary_base = 10000.0


def activate(gate_pre, up_pre):
    gate_clip = jnp.minimum(gate_pre, clamp_limit)
    up_clip = jnp.clip(up_pre, -clamp_limit, clamp_limit)
    return gate_clip * jax.nn.sigmoid(swish_alpha * gate_clip) * (up_clip + 1.0)


QUARTERS = 4
CORES = 2
MESH = pl.DeviceIdType.MESH


def regroup(capacity):
    rows = 4 * QUARTERS * capacity
    table = np.zeros((rows, rows), np.float32)
    for block in range(4):
        for part in range(QUARTERS):
            for row in range(capacity):
                table[
                    (part * 4 + block) * capacity + row, (block * QUARTERS + part) * capacity + row
                ] = 1.0
    return table


def in_three(value):
    first = value.astype(jnp.bfloat16)
    rest = value - first.astype(jnp.float32)
    second = rest.astype(jnp.bfloat16)
    third = (rest - second.astype(jnp.float32)).astype(jnp.bfloat16)
    return (first, second, third)


def lanes_of(shape):
    return lax.broadcasted_iota(jnp.int32, shape, len(shape) - 1)


def rows_of(shape):
    return lax.broadcasted_iota(jnp.int32, shape, 0)


def dot_f32(a, b, contract):
    return lax.dot_general(a, b, (contract, ((), ())), preferred_element_type=jnp.float32)


def layer_kernel(
    chips,
    decay_wide,
    decay_narrow,
    near_hbm,
    block_turns,
    gain,
    routes,
    route_weights,
    perm,
    perm_back,
    query_wide_hbm,
    key_wide_hbm,
    value_wide_hbm,
    query_narrow_hbm,
    key_narrow_hbm,
    value_narrow_hbm,
    out_wide_hbm,
    out_narrow_hbm,
    residual_hbm,
    gate_hbm,
    up_hbm,
    down_hbm,
    out,
    query_wide,
    key_wide,
    value_wide,
    query_narrow,
    key_narrow,
    value_narrow,
    out_wide,
    out_narrow,
    residual,
    gate,
    up,
    down,
    near,
    hidden,
    parted,
    chosen,
    picks,
    send,
    back,
    qbuf,
    kbuf,
    inner,
    mixed,
    pieces,
    arrived,
    answers,
    states,
    proj_a,
    far_a,
    sum_a,
    proj_b,
    far_b,
    sum_b,
    send_scale,
    gscale,
    gbuf,
    xbuf,
    hbuf,
    pbuf,
    rbuf,
    sbuf,
    ret,
    load_sem,
    p1s,
    p1r,
    p2s,
    p2r,
    pds,
    pdr,
    pes,
    per,
    zs,
    zr,
    xs,
    xr,
    ys,
    yr,
    ds,
    dr,
    es,
    er,
    rs,
    rr,
):
    z = lax.axis_index("sp_0")
    c = lax.axis_index("sp_1")
    x = lax.axis_index("tp")
    nx = lax.axis_size("tp")
    devices = chips * CORES
    me = z * CORES + c
    right = lax.rem(x + 1, nx)
    left = lax.rem(x + nx - 1, nx)
    length = query_wide.shape[0]
    units = 4
    lane = HEAD_WIDE
    block = min(128, length)
    f32 = jnp.float32
    bf16 = jnp.bfloat16

    def peer(step):
        other = lax.rem(me + step, devices)
        return other, {"sp_0": other // CORES, "sp_1": lax.rem(other, CORES)}

    def at_x(xt):
        return {"tp": xt}

    loads = [
        pltpu.make_async_copy(source, target, load_sem.at[n])
        for n, (source, target) in enumerate(
            (
                (near_hbm, near),
                (key_wide_hbm, key_wide),
                (key_narrow_hbm, key_narrow),
                (value_wide_hbm, value_wide),
                (value_narrow_hbm, value_narrow),
                (query_wide_hbm, query_wide),
                (query_narrow_hbm, query_narrow),
                (out_wide_hbm, out_wide),
                (out_narrow_hbm, out_narrow),
                (residual_hbm, residual),
                (gate_hbm, gate),
                (up_hbm, up),
                (down_hbm, down),
            )
        )
    ]
    for load in loads[:7]:
        load.start()

    barrier = pltpu.get_barrier_semaphore()
    pl.semaphore_signal(barrier, inc=1, device_id=at_x(right), device_id_type=MESH)
    pl.semaphore_signal(barrier, inc=1, device_id=at_x(left), device_id_type=MESH)

    @pl.loop(1, devices)
    def _(step):
        pl.semaphore_signal(barrier, inc=1, device_id=peer(step)[1], device_id_type=MESH)

    square = (length, length)
    below = (rows_of(square) >= lanes_of(square)).astype(f32).astype(bf16)
    decay_t = jnp.concatenate(
        [decay_wide[...], decay_narrow[...], jnp.zeros((2, length), f32)], axis=0
    )
    terms = in_three(decay_t)
    cum = sum(dot_f32(below, term, ((1,), (1,))) for term in terms)
    cum_t = sum(dot_f32(term, below, ((1,), (1,))) for term in terms)

    table_lane = lanes_of((length, lane))
    loads[0].wait()
    start = block_turns[me]
    start_cos = start[:, :lane]
    start_sin = start[:, lane:]
    cos_all = near[:, :lane] * start_cos - near[:, lane:] * start_sin
    sin_all = near[:, lane:] * start_cos + near[:, :lane] * start_sin
    low = table_lane < HEAD_WIDE // 2

    def wide_table(table):
        return jnp.where(low, table, pltpu.roll(table, HEAD_WIDE // 2, 1))

    def narrow_table(table):
        first = pltpu.roll(table, 64, 1)
        twice = jnp.where(table_lane < 32, first, pltpu.roll(first, 32, 1))
        return jnp.where(low, twice, pltpu.roll(twice, 64, 1))

    wide_cos = wide_table(cos_all)
    wide_sin = wide_table(sin_all)
    wide_sin = jnp.where(low, -wide_sin, wide_sin)
    narrow_cos = narrow_table(cos_all)
    narrow_sin = narrow_table(sin_all)
    narrow_low = lax.rem(table_lane, HEAD_NARROW) < HEAD_NARROW // 2
    narrow_sin = jnp.where(narrow_low, -narrow_sin, narrow_sin)

    def turned(source, unit):
        wide = unit < 2
        lanes = slice((unit % 2) * lane, (unit % 2 + 1) * lane)
        values = source[:, lanes].astype(f32)
        if wide:
            return values * wide_cos + pltpu.roll(values, HEAD_WIDE // 2, 1) * wide_sin
        swapped = jnp.where(
            narrow_low,
            pltpu.roll(values, lane - HEAD_NARROW // 2, 1),
            pltpu.roll(values, HEAD_NARROW // 2, 1),
        )
        return values * narrow_cos + swapped * narrow_sin

    def values_of(unit):
        source = value_wide if unit < 2 else value_narrow
        return source[:, (unit % 2) * lane : (unit % 2 + 1) * lane]

    def heads_of(unit):
        return (unit,) if unit < 2 else (2 * unit - 2, 2 * unit - 1)

    def per_lane(unit, column):
        heads = heads_of(unit)
        if len(heads) == 1:
            return column(heads[0])
        shape = (column(heads[0]).shape[0], lane)
        return jnp.where(lanes_of(shape) < HEAD_NARROW, column(heads[0]), column(heads[1]))

    def total_of(head):
        return cum_t[head : head + 1, length - 1 : length]

    unit_shape = (lane, lane)
    unit_low_row = rows_of(unit_shape) < HEAD_NARROW
    unit_low_lane = lanes_of(unit_shape) < HEAD_NARROW
    for load in loads[1:5]:
        load.wait()
    local = []
    for unit in range(units):
        width = HEAD_WIDE if unit < 2 else HEAD_NARROW
        key = (turned(key_wide if unit < 2 else key_narrow, unit) * width ** (-0.5)).astype(bf16)
        kbuf[unit] = key
        weight = per_lane(unit, lambda h: jnp.exp(total_of(h) - cum[:, h : h + 1]))
        weighted = (key.astype(f32) * weight).astype(bf16)
        state = dot_f32(weighted, values_of(unit), ((0,), (0,)))
        if unit < 2:
            local.append(state)
        else:
            packed = jnp.where(unit_low_row, state, pltpu.roll(state, HEAD_NARROW, 1))
            wide_total = total_of(unit - 2)
            narrow_total = jnp.where(
                unit_low_row, total_of(heads_of(unit)[0]), total_of(heads_of(unit)[1])
            )
            lane_id = lanes_of(unit_shape)
            for position, term in enumerate(
                in_three(jnp.broadcast_to(wide_total, unit_shape)) + in_three(narrow_total)
            ):
                packed = jnp.where(
                    lane_id == HEAD_NARROW + position, term.astype(f32), packed
                )
            local.append(packed)
    piece_rows = 2 * lane // devices
    for unit in range(units):
        here = slice((unit % 2) * (devices // 2), (unit % 2 + 1) * (devices // 2))
        lanes = slice((unit // 2) * lane, (unit // 2 + 1) * lane)
        pieces[here, :, lanes] = local[unit].reshape(devices // 2, piece_rows, lane).astype(bf16)

    pl.semaphore_wait(barrier, 2 + devices - 1)

    def piece_out(step):
        other, where = peer(step)
        return pltpu.make_async_remote_copy(
            src_ref=pieces.at[other],
            dst_ref=arrived.at[me],
            send_sem=p1s.at[step],
            recv_sem=p1r.at[step],
            device_id=where,
            device_id_type=MESH,
        )

    def answer_out(step):
        other, where = peer(step)
        return pltpu.make_async_remote_copy(
            src_ref=answers.at[other],
            dst_ref=states.at[me],
            send_sem=p2s.at[step],
            recv_sem=p2r.at[step],
            device_id=where,
            device_id_type=MESH,
        )

    @pl.loop(1, devices)
    def _(step):
        piece_out(step).start()

    for load in loads[7:]:
        load.start()
    arrived[me] = pieces[me]

    for load in loads[5:7]:
        load.wait()
    for unit in range(units):
        qbuf[unit] = turned(query_wide if unit < 2 else query_narrow, unit).astype(bf16)

    def within(unit):
        for start in range(0, length, block):
            stop = start + block
            shape = (block, stop)
            causal = rows_of(shape) + start >= lanes_of(shape)
            query = qbuf[unit, start:stop]
            key = kbuf[unit, :stop]
            value = values_of(unit)[:stop]
            outs = []
            for n, head in enumerate(heads_of(unit)):
                own = query
                if unit >= 2:
                    mine = lax.div(lanes_of((block, lane)), HEAD_NARROW) == n
                    own = jnp.where(mine, query.astype(f32), 0.0).astype(bf16)
                scores = dot_f32(own, key, ((1,), (1,)))
                gaps = cum[start:stop, head : head + 1] - cum_t[head : head + 1, :stop]
                faded = scores * jnp.exp(jnp.where(causal, gaps, -jnp.inf))
                outs.append(dot_f32(faded.astype(bf16), value, ((1,), (0,))))
            if unit >= 2:
                outs = [jnp.where(lanes_of((block, lane)) < HEAD_NARROW, outs[0], outs[1])]
            inner[unit, start:stop] = outs[0]

    for unit in range(2):
        within(unit)

    @pl.loop(1, devices)
    def _(step):
        piece_out(step).wait_recv()

    running = jnp.zeros((piece_rows, 2 * lane), f32)
    piece_lane = lanes_of((piece_rows, lane))
    for source in range(devices):
        answers[source] = running.astype(bf16)
        came = arrived[source].astype(f32)
        tail = came[:, lane:]

        def log_at(first):
            terms = (piece_lane >= first) & (piece_lane < first + 3)
            return jnp.sum(jnp.where(terms, tail, 0.0), axis=1, keepdims=True)

        scale = jnp.concatenate(
            [
                jnp.broadcast_to(jnp.exp(log_at(HEAD_NARROW)), piece_lane.shape),
                jnp.broadcast_to(jnp.exp(log_at(HEAD_NARROW + 3)), piece_lane.shape),
            ],
            axis=1,
        )
        running = scale * running + came

    @pl.loop(1, devices)
    def _(step):
        answer_out(step).start()

    states[me] = answers[me]

    for unit in range(2, units):
        within(unit)

    rows_dev = residual.shape[0]
    model_width = out_wide.shape[1]
    experts = devices
    one_hots = []
    for k in range(TOP_K):
        wanted = jnp.broadcast_to(routes[k : k + 1, :], (experts, rows_dev))
        one_hots.append((wanted == rows_of((experts, rows_dev))).astype(f32))
    rows_square = (rows_dev, rows_dev)
    earlier = (rows_of(rows_square) < lanes_of(rows_square)).astype(f32).astype(bf16)
    diagonal = rows_of(rows_square) == lanes_of(rows_square)

    def stood_up(row):
        return jnp.sum(
            jnp.where(diagonal, jnp.broadcast_to(row, rows_square), 0.0), axis=1, keepdims=True
        )

    before = jnp.zeros((experts, 1), f32)
    parts = QUARTERS * rows_dev
    slots = send.shape[0] * send.shape[1]
    capacity = send.shape[1] // QUARTERS
    width = send.shape[2]
    picked_rows = []
    ranks = []
    places = []
    for k in range(TOP_K):
        ahead = dot_f32(one_hots[k].astype(bf16), earlier, ((1,), (0,))) + before
        rank = jnp.sum(ahead * one_hots[k], axis=0, keepdims=True)
        before = before + jnp.sum(one_hots[k], axis=1, keepdims=True)
        across = routes[k : k + 1, :].astype(f32) * float(QUARTERS * capacity) + rank
        place = stood_up(across)
        picked_rows.append(
            jnp.concatenate([across + float(q * capacity) for q in range(QUARTERS)], axis=1)
        )
        ranks.append(rank)
        places.append(place)
    step_rows = slots // 4

    @pl.loop(0, 4)
    def _(n):
        first = pl.multiple_of(n * step_rows, step_rows)
        slot = (rows_of((step_rows, parts)) + first).astype(f32)
        hit = (slot == picked_rows[0]) | (slot == picked_rows[1])
        chosen[pl.ds(first, step_rows)] = hit.astype(f32).astype(bf16)

    @pl.loop(1, devices)
    def _(step):
        answer_out(step).wait_recv()

    for unit in range(units):
        here = slice((unit % 2) * (devices // 2), (unit % 2 + 1) * (devices // 2))
        lanes = slice((unit // 2) * lane, (unit // 2 + 1) * lane)
        state = states[here, :, lanes].astype(f32).reshape(lane, lane)
        if unit >= 2:
            state = jnp.where(
                unit_low_row,
                jnp.where(unit_low_lane, state, 0.0),
                jnp.where(unit_low_lane, 0.0, pltpu.roll(state, HEAD_NARROW, 1)),
            )
        carried = dot_f32(qbuf[unit], state.astype(bf16), ((1,), (0,)))
        kept = per_lane(unit, lambda h: jnp.exp(cum[:, h : h + 1]))
        value = inner[unit] + kept * carried

        def mean_of(entries):
            if unit < 2:
                return jnp.mean(entries, axis=1, keepdims=True)
            first = jnp.sum(jnp.where(low, entries, 0.0), axis=1, keepdims=True)
            second = jnp.sum(jnp.where(low, 0.0, entries), axis=1, keepdims=True)
            return jnp.where(low, first, second) * (1.0 / HEAD_NARROW)

        centered = value - mean_of(value)
        spread = mean_of(centered * centered)
        mixed[:, unit * lane : (unit + 1) * lane] = (
            centered * lax.rsqrt(spread + norm_eps)
        ).astype(bf16)

    half_model = model_width // 2
    first_cols = model_width // 4
    sub_width = width // 4
    starts = (0, first_cols)
    halves = (first_cols // 2, (model_width - first_cols) // 2)
    sums = ((proj_a, far_a, sum_a), (proj_b, far_b, sum_b))
    for load in loads[7:10]:
        load.wait()

    def x_copy(src, dst, send_sem, recv_sem, side):
        return pltpu.make_async_remote_copy(
            src_ref=src,
            dst_ref=dst,
            send_sem=send_sem,
            recv_sem=recv_sem,
            device_id=at_x(right if side == 0 else left),
            device_id_type=MESH,
        )

    def proj_far_half(n, side):
        return x_copy(
            sums[n][0].at[3, side], sums[n][1].at[side], pds.at[n, side], pdr.at[n, side], side
        )

    def proj_plain_half(n, side):
        return x_copy(
            sums[n][0].at[2 - side, 1 - side],
            sums[n][2].at[side, 1 - side],
            pes.at[n, side, 0],
            per.at[n, side, 0],
            side,
        )

    def proj_added_half(n, side):
        return x_copy(
            sums[n][0].at[2 - side, side],
            sums[n][2].at[side, side],
            pes.at[n, side, 1],
            per.at[n, side, 1],
            side,
        )

    def project(n, part, side):
        target = (x, left, right, lax.rem(x + 2, nx))[part]
        own_rows = pl.ds(pl.multiple_of(target * rows_dev, rows_dev), rows_dev)
        step = min(256, halves[n])

        @pl.loop(0, halves[n] // step)
        def _(i):
            cols = pl.ds(pl.multiple_of(starts[n] + side * halves[n] + i * step, step), step)
            here = pl.ds(pl.multiple_of(i * step, step), step)
            both = jnp.dot(
                mixed[own_rows, : 2 * lane], out_wide[:, cols], preferred_element_type=f32
            ) + jnp.dot(
                mixed[own_rows, 2 * lane :], out_narrow[:, cols], preferred_element_type=f32
            )
            sums[n][0][part, side, :, here] = both.astype(bf16)

    def add_far(n):
        own = sums[n][0]
        for side in range(2):
            proj_far_half(n, side).wait_recv()
            own[2 - side, side] = (
                own[2 - side, side].astype(f32) + sums[n][1][side].astype(f32)
            ).astype(bf16)
            proj_added_half(n, side).start()

    def finish_sum(n):
        own, _, came = sums[n]
        squares = jnp.zeros((rows_dev, 1), f32)
        for side in range(2):
            proj_plain_half(n, side).wait_recv()
            proj_added_half(n, side).wait_recv()
        for h in range(2):
            cols = slice(starts[n] + h * halves[n], starts[n] + (h + 1) * halves[n])
            stream = residual[:, cols].astype(f32) + (
                own[0, h].astype(f32) + came[0, h].astype(f32) + came[1, h].astype(f32)
            )
            hidden[:, cols] = stream
            squares = squares + jnp.sum(stream * stream, axis=1, keepdims=True)
        return squares

    step_experts = experts // 4

    def fill_send(n):
        here = slice(0, sub_width) if n == 0 else slice(sub_width, width)
        size = sub_width if n == 0 else width - sub_width
        for q in range(QUARTERS):
            cols = slice(starts[n] + q * size, starts[n] + (q + 1) * size)
            parted[q * rows_dev : (q + 1) * rows_dev, here] = (
                hidden[:, cols] * gain[:, cols]
            ).astype(bf16)

        @pl.loop(0, 4)
        def _(i):
            first = pl.multiple_of(i * step_rows, step_rows)
            taken = jnp.dot(
                chosen[pl.ds(first, step_rows)], parted[:, here], preferred_element_type=f32
            ).astype(bf16)
            send[pl.ds(i * step_experts, step_experts), :, here] = taken.reshape(
                step_experts, QUARTERS * capacity, size
            )

    half = chips // 2
    groups = half
    last = groups - 1
    block_rows = send.shape[1]
    rows = 4 * capacity
    hidden_width = gate.shape[1]

    def remote(src, dst, send_sem, recv_sem, to):
        return pltpu.make_async_remote_copy(
            src_ref=src,
            dst_ref=dst,
            send_sem=send_sem,
            recv_sem=recv_sem,
            device_id=to,
            device_id_type=MESH,
        )

    def at_z(zt, ct):
        return {"sp_0": zt, "sp_1": ct}

    def chip_at(offset):
        return lax.rem(z + offset + chips, chips)

    def parts_of(piece, sender, taker):
        if piece == 2:
            return send_scale.at[sender], gscale.at[taker]
        lanes = pl.ds(0, sub_width) if piece == 0 else pl.ds(sub_width, width - sub_width)
        return send.at[sender, :, lanes], gbuf.at[taker + (slice(None), lanes)]

    def partner_out(piece):
        src, dst = parts_of(piece, z * CORES + 1 - c, (0, last, c))
        return remote(src, dst, zs.at[piece, 4 * last], zr.at[piece, 4 * last], at_z(z, 1 - c))

    def far_out(piece, ct):
        zt = chip_at(half)
        src, dst = parts_of(piece, zt * CORES + ct, (0, last, 2 + c))
        return remote(
            src, dst, zs.at[piece, 4 * last + 2 + ct], zr.at[piece, 4 * last + 2 + c], at_z(zt, ct)
        )

    def near_out(piece, d, sign, ct):
        zt = chip_at(d) if sign == 0 else chip_at(-d)
        src, dst = parts_of(piece, zt * CORES + ct, (0, d - 1, 2 * sign + c))
        return remote(
            src,
            dst,
            zs.at[piece, 4 * (d - 1) + 2 * sign + ct],
            zr.at[piece, 4 * (d - 1) + 2 * sign + c],
            at_z(zt, ct),
        )

    def dispatch(pieces_now):
        for piece in pieces_now:
            partner_out(piece).start()

        @pl.loop(1, half)
        def _(d):
            for ct in range(CORES):
                for sign in range(2):
                    for piece in pieces_now:
                        near_out(piece, d, sign, ct).start()

        for ct in range(CORES):
            for piece in pieces_now:
                far_out(piece, ct).start()

    for side in range(2):
        project(0, 3, side)
        proj_far_half(0, side).start()
    for side in range(2):
        project(0, 2 - side, 1 - side)
        proj_plain_half(0, side).start()
    for side in range(2):
        project(0, 2 - side, side)
    for side in range(2):
        project(1, 3, side)
    add_far(0)
    for side in range(2):
        proj_far_half(1, side).start()
    for side in range(2):
        project(1, 2 - side, 1 - side)
        proj_plain_half(1, side).start()
    for side in range(2):
        project(0, 0, side)
    squares = finish_sum(0)
    fill_send(0)
    dispatch((0,))
    for side in range(2):
        project(1, 2 - side, side)
    add_far(1)
    for side in range(2):
        project(1, 0, side)
    squares = squares + finish_sum(1)
    scale_row = lax.rsqrt(squares * (1.0 / model_width) + norm_eps)
    laid = jnp.sum(
        jnp.where(diagonal, jnp.broadcast_to(scale_row, rows_square), 0.0), axis=0, keepdims=True
    )
    slot_scale = jnp.zeros((experts, lane), f32)
    for k in range(TOP_K):
        at_rank = jnp.broadcast_to(stood_up(ranks[k]), (rows_dev, lane)) == lanes_of(
            (rows_dev, lane)
        ).astype(f32)
        for term in in_three(laid):
            held = (one_hots[k] * term.astype(f32)).astype(bf16)
            slot_scale = slot_scale + dot_f32(
                held, at_rank.astype(f32).astype(bf16), ((1,), (0,))
            )
    for e in range(experts):
        send_scale[e] = slot_scale[e : e + 1]
    fill_send(1)
    dispatch((2, 1))
    gbuf[0, last, c] = send[me]
    gscale[0, last, c] = send_scale[me]
    for k in range(TOP_K):
        for q in range(QUARTERS):
            own = slice(q * rows_dev, (q + 1) * rows_dev)
            wanted = jnp.broadcast_to(places[k] + float(q * capacity), (rows_dev, slots))
            picks[k, own] = (
                (wanted == lanes_of((rows_dev, slots)).astype(f32)).astype(f32).astype(bf16)
            )
    for load in loads[10:]:
        load.wait()

    def z_arrived(piece, g, j):
        src, dst = parts_of(piece, 0, (0, g, j))
        return remote(src, dst, zs.at[piece, 0], zr.at[piece, 4 * g + j], at_z(z, 1 - c))

    def spread(kind, side, g):
        held = (gbuf, gscale)[kind]
        return remote(
            held.at[0, g],
            held.at[1 + side, g],
            xs.at[kind, side, g],
            xr.at[kind, side, g],
            at_x(right if side == 0 else left),
        )

    def relay(kind, side, g):
        held = (gbuf, gscale)[kind]
        return remote(
            held.at[1 + side, g, pl.ds(2 * side, 2)],
            held.at[3, g, pl.ds(2 * side, 2)],
            ys.at[kind, side, g],
            yr.at[kind, side, g],
            at_x(right if side == 0 else left),
        )

    def stage_a(g):
        @pl.when(g < last)
        def _():
            for piece in range(3):
                for j in range(4):
                    z_arrived(piece, g, j).wait_recv()

        @pl.when(g == last)
        def _():
            for piece in range(3):
                for j in (0, 2, 3):
                    z_arrived(piece, g, j).wait_recv()

        for side in range(2):
            for kind in range(2):
                spread(kind, side, g).start()

    def stage_b(g):
        for side in range(2):
            for kind in range(2):
                spread(kind, side, g).wait_recv()
                relay(kind, side, g).start()

    def far_half(side, g):
        return remote(
            pbuf.at[g, 3, side],
            rbuf.at[side, g],
            ds.at[side, g],
            dr.at[side, g],
            at_x(right if side == 0 else left),
        )

    def plain_half(side, g):
        return remote(
            pbuf.at[g, 2 - side, 1 - side],
            sbuf.at[side, 1 - side, g],
            es.at[side, 0, g],
            er.at[side, 0, g],
            at_x(right if side == 0 else left),
        )

    def added_half(side, g):
        return remote(
            pbuf.at[g, 2 - side, side],
            sbuf.at[side, side, g],
            es.at[side, 1, g],
            er.at[side, 1, g],
            at_x(right if side == 0 else left),
        )

    def stage_c(g):
        for side in range(2):
            for kind in range(2):
                relay(kind, side, g).wait_recv()
        factors = []
        factor_shape = (rows, lane)
        for part in range(4):
            block = gbuf[part, g].reshape(4 * block_rows, width)
            turned_rows = jnp.dot(perm[...], block, preferred_element_type=jnp.float32).astype(
                jnp.bfloat16
            )
            rest = width - sub_width
            for q in range(QUARTERS):
                taken = turned_rows[q * rows : (q + 1) * rows]
                own = pl.ds(part * rows, rows)
                xbuf[own, pl.ds(q * sub_width, sub_width)] = taken[:, :sub_width]
                xbuf[own, pl.ds(first_cols + q * rest, rest)] = taken[:, sub_width:]
            factor = jnp.zeros((rows, 1), f32)
            for j in range(4):
                place_in = rows_of(factor_shape) - j * capacity
                mine = (lanes_of(factor_shape) == place_in) & (place_in < capacity)
                came = jnp.broadcast_to(gscale[part, g, j], factor_shape)
                factor = factor + jnp.sum(jnp.where(mine, came, 0.0), axis=1, keepdims=True)
            factors.append(factor)
        factor = jnp.concatenate(factors, axis=0)
        step = min(256, hidden_width)

        @pl.loop(0, hidden_width // step)
        def _(n):
            cols = pl.ds(pl.multiple_of(n * step, step), step)
            gate_pre = jnp.dot(xbuf[...], gate[:, cols], preferred_element_type=jnp.float32)
            up_pre = jnp.dot(xbuf[...], up[:, cols], preferred_element_type=jnp.float32)
            hbuf[:, cols] = activate(factor * gate_pre, factor * up_pre).astype(jnp.bfloat16)

        out_step = min(512, half_model)

        @pl.loop(0, half_model // out_step)
        def _(n):
            for side in range(2):
                cols = pl.ds(
                    pl.multiple_of(side * half_model + n * out_step, out_step), out_step
                )
                here = pl.ds(pl.multiple_of(n * out_step, out_step), out_step)
                part_sum = jnp.dot(
                    hbuf[...], down[:, cols], preferred_element_type=jnp.float32
                ).astype(jnp.bfloat16)
                for part in range(4):
                    pbuf[g, part, side, :, here] = part_sum[part * rows : (part + 1) * rows]

        for side in range(2):
            far_half(side, g).start()
        for side in range(2):
            plain_half(side, g).start()

    def stage_e(g):
        for side in range(2):
            far_half(side, g).wait_recv()
            pbuf[g, 2 - side, side] = (
                pbuf[g, 2 - side, side].astype(jnp.float32) + rbuf[side, g].astype(jnp.float32)
            ).astype(jnp.bfloat16)
            added_half(side, g).start()

    def stage_f(g):
        for side in range(2):
            plain_half(side, g).wait_recv()
            added_half(side, g).wait_recv()
        quarters = []
        for h in range(2):
            total = (
                pbuf[g, 0, h].astype(jnp.float32)
                + sbuf[0, h, g].astype(jnp.float32)
                + sbuf[1, h, g].astype(jnp.float32)
            ).astype(jnp.bfloat16)
            quarters += [total[:, :width], total[:, width:]]
        stacked = jnp.concatenate(quarters, axis=0)
        ret[g] = (
            jnp.dot(perm_back[...], stacked, preferred_element_type=jnp.float32)
            .astype(jnp.bfloat16)
            .reshape(4, block_rows, width)
        )

    def near_back(g, sign, cs):
        zt = chip_at(-g - 1) if sign == 0 else chip_at(g + 1)
        return remote(
            ret.at[g, 2 * sign + cs],
            back.at[me],
            rs.at[4 * g + 2 * sign + cs],
            rr.at[4 * g + 2 * sign + c],
            at_z(zt, cs),
        )

    def far_back(cs):
        return remote(
            ret.at[last, 2 + cs],
            back.at[me],
            rs.at[4 * last + 2 + cs],
            rr.at[4 * last + 2 + c],
            at_z(chip_at(half), cs),
        )

    def partner_back():
        return remote(
            ret.at[last, 1 - c], back.at[me], rs.at[4 * last], rr.at[4 * last], at_z(z, 1 - c)
        )

    def stage_h(g):
        @pl.when(g < last)
        def _():
            for cs in range(CORES):
                for sign in range(2):
                    near_back(g, sign, cs).start()

        @pl.when(g == last)
        def _():
            for cs in range(CORES):
                far_back(cs).start()
            partner_back().start()
            back[me] = ret[last, c]

    @pl.loop(0, groups + 4)
    def _(i):
        @pl.when(i >= 4)
        def _():
            stage_f(i - 4)

        @pl.when(i >= 4)
        def _():
            stage_h(i - 4)

        @pl.when((i >= 3) & (i < groups + 3))
        def _():
            stage_e(i - 3)

        @pl.when((i >= 2) & (i < groups + 2))
        def _():
            stage_c(i - 2)

        @pl.when((i >= 1) & (i < groups + 1))
        def _():
            stage_b(i - 1)

        @pl.when(i < groups)
        def _():
            stage_a(i)

    for piece in range(3):
        partner_out(piece).wait_send()
        for ct in range(CORES):
            far_out(piece, ct).wait_send()
    partner_back().wait_send()
    partner_back().wait_recv()
    for ct in range(CORES):
        far_back(ct).wait_send()

    def back_arrived(g, j):
        return remote(ret.at[0, 0], back.at[0], rs.at[0], rr.at[4 * g + j], at_z(z, 1 - c))

    for j in (2, 3):
        back_arrived(last, j).wait_recv()

    @pl.loop(0, last)
    def _(g):
        for sign in range(2):
            for ct in range(CORES):
                for piece in range(3):
                    near_out(piece, g + 1, sign, ct).wait_send()
                near_back(g, sign, ct).wait_send()
        for j in range(4):
            back_arrived(g, j).wait_recv()

    @pl.loop(0, groups)
    def _(g):
        for side in range(2):
            for kind in range(2):
                spread(kind, side, g).wait_send()
                relay(kind, side, g).wait_send()
            far_half(side, g).wait_send()
            plain_half(side, g).wait_send()
            added_half(side, g).wait_send()

    arrived_rows = back[...].reshape(slots, width)
    shares = [stood_up(route_weights[k : k + 1, :]) for k in range(TOP_K)]
    for q in range(QUARTERS):
        own = slice(q * rows_dev, (q + 1) * rows_dev)
        cols = slice(q * width, (q + 1) * width)
        total = hidden[:, cols]
        for k in range(TOP_K):
            total = total + shares[k] * jnp.dot(
                picks[k, own], arrived_rows, preferred_element_type=f32
            )
        out[:, cols] = total

    @pl.loop(1, devices)
    def _(step):
        piece_out(step).wait_send()
        answer_out(step).wait_send()

    for n in range(2):
        for side in range(2):
            proj_far_half(n, side).wait_send()
            proj_plain_half(n, side).wait_send()
            proj_added_half(n, side).wait_send()


def turn_tables(length, blocks):
    inverse = [
        rotary_base ** (-np.arange(size // 2) / (size // 2)) for size in (HEAD_WIDE, HEAD_NARROW)
    ]
    inverse = np.concatenate(inverse + [np.zeros(HEAD_NARROW // 2)])

    def table(positions):
        angles = positions[:, None] * inverse[None, :]
        return jnp.asarray(
            np.concatenate([np.cos(angles), np.sin(angles)], axis=1), jnp.float32
        )

    return table(np.arange(length)), table(np.arange(blocks) * length)[:, None, :]


def layer_stage(
    query_wide,
    key_wide,
    value_wide,
    decay_wide,
    query_narrow,
    key_narrow,
    value_narrow,
    decay_narrow,
    residual,
    out_wide,
    out_narrow,
    norm_gain,
    routes,
    route_weights,
    gate,
    up,
    down,
):
    length = query_wide.shape[0]
    chips = lax.axis_size("sp_0")
    devices = chips * CORES
    groups = chips // 2
    rows_dev, model_width = residual.shape
    width = model_width // QUARTERS
    hidden_width = gate.shape[1]
    capacity = max(2, 3 * rows_dev * TOP_K // (2 * devices))
    block_rows = QUARTERS * capacity
    rows = 4 * capacity
    slots = devices * block_rows
    table = regroup(capacity)
    near, block_turns = turn_tables(length, devices)
    vmem = pl.BlockSpec(memory_space=pltpu.VMEM)
    hbm = pl.BlockSpec(memory_space=pl.ANY)
    bf16 = jnp.bfloat16
    f32 = jnp.float32
    dma = pltpu.SemaphoreType.DMA
    piece_rows = 2 * HEAD_WIDE // devices
    moved = pltpu.VMEM((devices, piece_rows, 2 * HEAD_WIDE), bf16)
    heads = pltpu.VMEM(query_wide.shape, bf16)
    half = model_width // 2
    from_hbm = (
        query_wide,
        key_wide,
        value_wide,
        query_narrow,
        key_narrow,
        value_narrow,
        out_wide,
        out_narrow,
        residual,
        gate,
        up,
        down,
    )
    return pl.pallas_call(
        functools.partial(layer_kernel, chips),
        out_shape=jax.ShapeDtypeStruct(residual.shape, f32),
        in_specs=[vmem] * 2 + [hbm] + [vmem] * 6 + [hbm] * 12,
        out_specs=vmem,
        scratch_shapes=[pltpu.VMEM(a.shape, bf16) for a in from_hbm]
        + [
            pltpu.VMEM(near.shape, f32),
            pltpu.VMEM((rows_dev, model_width), f32),
            pltpu.VMEM((QUARTERS * rows_dev, width), bf16),
            pltpu.VMEM((slots, QUARTERS * rows_dev), bf16),
            pltpu.VMEM((TOP_K, QUARTERS * rows_dev, slots), bf16),
            pltpu.VMEM((devices, block_rows, width), bf16),
            pltpu.VMEM((devices, block_rows, width), bf16),
            pltpu.VMEM((4, length, HEAD_WIDE), bf16),
            pltpu.VMEM((4, length, HEAD_WIDE), bf16),
            pltpu.VMEM((4, length, HEAD_WIDE), f32),
            pltpu.VMEM((length, 4 * HEAD_WIDE), bf16),
            moved,
            moved,
            moved,
            moved,
            pltpu.VMEM((4, 2, rows_dev, half // 4), bf16),
            pltpu.VMEM((2, rows_dev, half // 4), bf16),
            pltpu.VMEM((2, 2, rows_dev, half // 4), bf16),
            pltpu.VMEM((4, 2, rows_dev, half - half // 4), bf16),
            pltpu.VMEM((2, rows_dev, half - half // 4), bf16),
            pltpu.VMEM((2, 2, rows_dev, half - half // 4), bf16),
            pltpu.VMEM((devices, 1, HEAD_WIDE), f32),
            pltpu.VMEM((4, groups, 4, 1, HEAD_WIDE), f32),
            pltpu.VMEM((4, groups, 4, block_rows, width), bf16),
            pltpu.VMEM((4 * rows, model_width), bf16),
            pltpu.VMEM((4 * rows, hidden_width), bf16),
            pltpu.VMEM((groups, 4, 2, rows, half), bf16),
            pltpu.VMEM((2, groups, rows, half), bf16),
            pltpu.VMEM((2, 2, groups, rows, half), bf16),
            pltpu.VMEM((groups, 4, block_rows, width), bf16),
            dma((13,)),
            dma((devices,)),
            dma((devices,)),
            dma((devices,)),
            dma((devices,)),
            dma((2, 2)),
            dma((2, 2)),
            dma((2, 2, 2)),
            dma((2, 2, 2)),
            dma((3, 4 * groups)),
            dma((3, 4 * groups)),
            dma((2, 2, groups)),
            dma((2, 2, groups)),
            dma((2, 2, groups)),
            dma((2, 2, groups)),
            dma((2, groups)),
            dma((2, groups)),
            dma((2, 2, groups)),
            dma((2, 2, groups)),
            dma((4 * groups,)),
            dma((4 * groups,)),
        ],
        compiler_params=pltpu.CompilerParams(
            collective_id=0, has_side_effects=True, vmem_limit_bytes=60 * 1024 * 1024
        ),
        name="layer_stage",
    )(
        decay_wide.T,
        decay_narrow.T,
        near,
        block_turns,
        norm_gain[None, :],
        routes.T,
        route_weights.T,
        jnp.asarray(table, bf16),
        jnp.asarray(table.T, bf16),
        *from_hbm,
    ).astype(bf16)


def body(*arguments):
    return layer_stage(*arguments[:14], *(weight[0] for weight in arguments[14:]))


def solution(mesh):
    torus = Mesh(
        mesh.devices.reshape(mesh.shape["grp"], 16, 2, mesh.shape["tp"]),
        ("grp", "sp_0", "sp_1", "tp"),
    )
    in_specs = (
        P(GRP_SP, "tp"),
        P(GRP_SP, "tp"),
        P(GRP_SP, "tp"),
        P(GRP_SP, "tp"),
        P(GRP_SP, "tp"),
        P(GRP_SP, "tp"),
        P(GRP_SP, "tp"),
        P(GRP_SP, "tp"),
        P(GRP_SP_TP, None),
        P("tp", None),
        P("tp", None),
        P(),
        P(GRP_SP_TP, None),
        P(GRP_SP_TP, None),
        P(SP, None, "tp"),
        P(SP, None, "tp"),
        P(SP, "tp", None),
    )
    out_specs = P(GRP_SP_TP, None)
    return jax.shard_map(body, mesh=torus, in_specs=in_specs, out_specs=out_specs, check_vma=False)
```
